256 devices in a mesh: kv: 32 (over z, x), tp: 8 (over y, core).
Axes of the slice: x: 4, y: 4, z: 8, core: 2. Of those that a mesh axis runs over, the one named last changes fastest.
Arguments:
- tokens: bfloat16 [1024, 4096], P('kv', 'tp'), may hold values from -12 to 12
- norm_gain: float32 [4096], replicated, may hold values from 0.1 to 1.9
- query_weight: bfloat16 [4096, 4096], P('kv', 'tp'), may hold values from -0.09375 to 0.09375
- key_weight: bfloat16 [4096, 4096], P('kv', 'tp'), may hold values from -0.09375 to 0.09375
- value_weight: bfloat16 [4096, 4096], P('kv', 'tp'), may hold values from -0.09375 to 0.09375
- outgate_weight: bfloat16 [4096, 4096], P('kv', 'tp'), may hold values from -0.09375 to 0.09375
- ingate_weight: bfloat16 [4096, 16], replicated, may hold values from -0.09375 to 0.09375
- forget_weight: bfloat16 [4096, 16], replicated, may hold values from -0.09375 to 0.09375
- forget_bias: float32 [16], replicated, may hold values from 0.5 to 4
- output_weight: bfloat16 [4096, 4096], P('tp', 'kv'), may hold values from -0.09375 to 0.09375
- state_memory: float32 [256, 16, 256, 256], P('kv', 'tp'), may hold values from -0.8 to 0.8
- state_normaliser: float32 [256, 16, 256], P('kv', 'tp'), may hold values from -0.8 to 0.8
- state_stabiliser: float32 [256, 16], P('kv', 'tp'), may hold values from -4 to 4
- past_keys: bfloat16 [256, 4, 4096], P('kv', None, 'tp'), may hold values from -6 to 6
- past_values: bfloat16 [256, 4, 4096], P('kv', None, 'tp'), may hold values from -6 to 6
- past_ingate: float32 [256, 4, 16], P('kv', None, 'tp'), may hold values from -4 to 4
- past_forget: float32 [256, 4, 16], P('kv', None, 'tp'), may hold values from -1 to 4
- accepted: int32 [256], P('kv'), may hold values from 0 to 4
Outputs:
- mixed: bfloat16 [1024, 4096], P('kv', 'tp')
- taken_memory: float32 [256, 16, 256, 256], P('kv', 'tp')
- taken_normaliser: float32 [256, 16, 256], P('kv', 'tp')
- taken_stabiliser: float32 [256, 16], P('kv', 'tp')
- new_keys: bfloat16 [1024, 4096], P('kv', 'tp')
- new_values: bfloat16 [1024, 4096], P('kv', 'tp')
The draws below stay inside these ranges and needn't reach their ends.
All inputs are finite; a program needn't handle non-finite values.
Results may differ from the reference program's by a relative error of at most 0.03.
Values may be sent and summed in bfloat16 or wider, within the bound.
A program may use at most 64 MiB of HBM per device.

```python
import jax
import jax.numpy as jnp
from jax import lax

D = 4096
HEADS = 16
DK = 256
DV = 256
PROPS = 4
SEQS = 256
TOKENS = 1024
HD = 4096
N_TP = 8


def draw_tokens(key, part):
    base_key = jax.random.fold_in(key, 11)
    scale_key = jax.random.fold_in(key, 12)
    base_values = jnp.clip(jax.random.normal(base_key, (TOKENS, D), jnp.float32), -4.0, 4.0)
    levels = jax.random.uniform(scale_key, (TOKENS, 32), jnp.float32, jnp.log(0.3), jnp.log(3.0))
    block_scale = jnp.repeat(jnp.exp(levels), D // 32, axis=1)
    return (base_values * block_scale).astype(jnp.bfloat16)


def touch_ends(array, stream_key, smallest, top_value):
    index_at = [jax.random.randint(jax.random.fold_in(stream_key, axis), (), 0, length) for axis, length in enumerate(array.shape)]
    widest = array.shape.index(max(array.shape))
    beside = index_at[:widest] + [(index_at[widest] + 1) % array.shape[widest]] + index_at[widest + 1:]
    return array.at[tuple(index_at)].set(smallest).at[tuple(beside)].set(top_value)


def level_of(rng, shape, shards, least, high):
    def one(position, parts):
        steps = jax.random.uniform(jax.random.fold_in(jax.random.fold_in(rng, 6), position), (parts,), jnp.float32, least / len(shards), high / len(shards))
        return jnp.repeat(jnp.exp(steps), shape[position] // parts).reshape((-1,) + (1,) * (len(shape) - position - 1))

    gain = one(*shards[0])
    for cut in shards[1:]:
        gain = gain * one(*cut)
    return gain


def scatter_about(rng, dims, spread, most, pieces=(), held_as=jnp.bfloat16):
    array = jax.random.normal(rng, dims, jnp.float32) * spread
    if len(pieces) > 0:
        array = level_of(rng, dims, pieces, -0.22, 0.18) * array
    return jnp.clip(array, min=-most, max=most).astype(held_as)


def setup_inputs(seed: int = 0) -> dict:
    keys = jax.random.split(jax.random.key(seed), 19)
    tokens = draw_tokens(jax.random.fold_in(keys[18], 71), 0)
    norm_gain = jnp.clip(1.0 + 0.18 * jax.random.normal(keys[1], (D,), jnp.float32), 0.1, 1.9)
    query_weight = scatter_about(keys[2], (D, HD), D ** -0.5, 0.09375, ((0, 32), (1, 8)))
    key_weight = scatter_about(keys[3], (D, HD), D ** -0.5, 0.09375, ((0, 32), (1, 8)))
    value_weight = scatter_about(keys[4], (D, HD), D ** -0.5, 0.09375, ((0, 32), (1, 8)))
    outgate_weight = scatter_about(keys[5], (D, HD), D ** -0.5, 0.09375, ((0, 32), (1, 8)))
    ingate_weight = scatter_about(keys[6], (D, HEADS), D ** -0.5, 0.09375)
    forget_weight = scatter_about(keys[7], (D, HEADS), D ** -0.5, 0.09375)
    forget_bias = jnp.clip(jax.random.uniform(keys[8], (HEADS,), jnp.float32, 0.5, 4.0), 0.5, 4.0)
    output_weight = scatter_about(keys[9], (HD, D), HD ** -0.5, 0.09375, ((0, 8), (1, 32)))
    state_memory = scatter_about(keys[10], (SEQS, HEADS, DK, DV), 0.1, 0.8, ((0, 32), (1, 8)), jnp.float32)
    state_normaliser = scatter_about(keys[11], (SEQS, HEADS, DK), 0.1, 0.8, ((0, 32), (1, 8)), jnp.float32)
    state_stabiliser = scatter_about(keys[12], (SEQS, HEADS), 1.0, 4.0, ((0, 32), (1, 8)), jnp.float32)
    past_keys = scatter_about(keys[13], (SEQS, PROPS, HD), 1.0, 6.0, ((0, 32), (2, 8)))
    past_values = scatter_about(keys[14], (SEQS, PROPS, HD), 1.0, 6.0, ((0, 32), (2, 8)))
    past_ingate = scatter_about(keys[15], (SEQS, PROPS, HEADS), 1.0, 4.0, ((0, 32), (2, 8)), jnp.float32)
    past_forget = jnp.clip(-1.0 + 5.0 * jax.random.uniform(keys[16], (SEQS, PROPS, HEADS), jnp.float32) ** level_of(keys[16], (SEQS, PROPS, HEADS), ((0, 32), (2, 8)), -0.2, 0.2), -1.0, 4.0)
    accepted = touch_ends(jax.random.randint(keys[17], (SEQS,), 0, PROPS + 1), jax.random.fold_in(keys[17], 1), 0, PROPS).astype(jnp.int32)
    return dict(tokens=tokens, norm_gain=norm_gain, query_weight=query_weight, key_weight=key_weight, value_weight=value_weight, outgate_weight=outgate_weight, ingate_weight=ingate_weight, forget_weight=forget_weight, forget_bias=forget_bias, output_weight=output_weight, state_memory=state_memory, state_normaliser=state_normaliser, state_stabiliser=state_stabiliser, past_keys=past_keys, past_values=past_values, past_ingate=past_ingate, past_forget=past_forget, accepted=accepted)


exact_mode = lax.Precision.HIGHEST
epsilon = 1e-06

def rounded(values):
    return lax.optimization_barrier(values.astype(jnp.bfloat16))

def heads_view(rows, seq_count, head_count):
    shaped = rows.astype(jnp.float32).reshape(seq_count, -1, head_count, rows.shape[-1] // head_count)
    return shaped.transpose(0, 2, 1, 3)

def catch_up(memory, normaliser, stabiliser, key_rows, values, in_gate, forget_pre, taken_mask):
    log_forget = jnp.where(taken_mask, jax.nn.log_sigmoid(forget_pre), 0.0)
    running = jnp.cumsum(log_forget, axis=-1)
    chain_total = running[..., -1]
    end_logs = jnp.where(taken_mask, chain_total[..., None] - running + in_gate, -jnp.inf)
    stable_new = jnp.maximum(chain_total + stabiliser, lax.optimization_barrier(jnp.max(end_logs, axis=-1)))
    carry_decay = jnp.exp(chain_total + stabiliser - stable_new)
    weighted = key_rows * jnp.exp(end_logs - stable_new[..., None])[..., None]
    memory_new = carry_decay[..., None, None] * memory + jnp.einsum('...pd,...pe->...de', weighted, values, precision=exact_mode)
    normaliser_new = carry_decay[..., None] * normaliser + lax.optimization_barrier(jnp.sum(weighted, axis=-2))
    return (memory_new, normaliser_new, stable_new)

def advance(memory, normaliser, stabiliser, query_rows, key_rows, values, in_gate, forget_pre):
    chain_len = query_rows.shape[-2]
    running = jnp.cumsum(jax.nn.log_sigmoid(forget_pre), axis=-1)
    causal = jnp.arange(chain_len)[:, None] >= jnp.arange(chain_len)[None, :]
    within = jnp.where(causal, running[..., :, None] - running[..., None, :] + in_gate[..., None, :], -jnp.inf)
    carried = running + stabiliser[..., None]
    stable = jnp.maximum(carried, lax.optimization_barrier(jnp.max(within, axis=-1)))
    scores = jnp.einsum('...td,...sd->...ts', query_rows, key_rows, precision=exact_mode) * jnp.exp(within - stable[..., None])
    carry_weight = jnp.exp(carried - stable)
    numerator = carry_weight[..., None] * jnp.einsum('...td,...de->...te', query_rows, memory, precision=exact_mode)
    numerator = numerator + jnp.einsum('...ts,...se->...te', scores, values, precision=exact_mode)
    denominator = carry_weight * jnp.einsum('...td,...d->...t', query_rows, normaliser, precision=exact_mode) + lax.optimization_barrier(jnp.sum(scores, axis=-1))
    return numerator / jnp.maximum(jnp.abs(denominator), 1.0)[..., None]

def reference(tokens, norm_gain, query_weight, key_weight, value_weight, outgate_weight, ingate_weight, forget_weight, forget_bias, output_weight, state_memory, state_normaliser, state_stabiliser, past_keys, past_values, past_ingate, past_forget, accepted):
    floats = tokens.astype(jnp.float32)
    squares = lax.optimization_barrier(jnp.sum(floats * floats, axis=1, keepdims=True))
    normed = (floats * lax.rsqrt(squares / D + epsilon) * norm_gain).astype(jnp.bfloat16)
    query_b = rounded(jnp.dot(normed, query_weight, preferred_element_type=jnp.float32))
    key_b = rounded(jnp.dot(normed, key_weight, preferred_element_type=jnp.float32))
    value_b = rounded(jnp.dot(normed, value_weight, preferred_element_type=jnp.float32))
    outgate_b = rounded(jnp.dot(normed, outgate_weight, preferred_element_type=jnp.float32))
    in_gate = jnp.dot(normed, ingate_weight, preferred_element_type=jnp.float32)
    forget_pre = jnp.dot(normed, forget_weight, preferred_element_type=jnp.float32) + forget_bias
    seq_count = past_keys.shape[0]
    chain_len = past_keys.shape[1]
    key_scale = DK ** (-0.5)
    query_h = heads_view(query_b, seq_count, HEADS)
    key_h = heads_view(key_b, seq_count, HEADS) * key_scale
    value_h = heads_view(value_b, seq_count, HEADS)
    outgate_h = heads_view(outgate_b, seq_count, HEADS)
    in_h = in_gate.reshape(seq_count, chain_len, HEADS).transpose(0, 2, 1)
    forget_h = forget_pre.reshape(seq_count, chain_len, HEADS).transpose(0, 2, 1)
    past_key_h = heads_view(past_keys, seq_count, HEADS) * key_scale
    past_value_h = heads_view(past_values, seq_count, HEADS)
    past_in_h = past_ingate.transpose(0, 2, 1)
    past_forget_h = past_forget.transpose(0, 2, 1)

    def per_sequence(items):
        memory, normaliser, stabiliser, query_s, key_s, value_s, outgate_s, in_s, forget_s, past_key_s, past_value_s, past_in_s, past_forget_s, taken_count = items
        taken_mask = (jnp.arange(chain_len) < taken_count)[None, :]
        memory_new, normaliser_new, stable_new = catch_up(memory, normaliser, stabiliser, past_key_s, past_value_s, past_in_s, past_forget_s, taken_mask)
        hidden = advance(memory_new, normaliser_new, stable_new, query_s, key_s, value_s, in_s, forget_s)
        gated = (jax.nn.sigmoid(outgate_s) * hidden).transpose(1, 0, 2).reshape(chain_len, -1).astype(jnp.bfloat16)
        return (memory_new, normaliser_new, stable_new, gated)
    memory_out, normaliser_out, stable_out, gated_all = lax.map(per_sequence, (state_memory, state_normaliser, state_stabiliser, query_h, key_h, value_h, outgate_h, in_h, forget_h, past_key_h, past_value_h, past_in_h, past_forget_h, accepted))
    gated_rows = gated_all.reshape(seq_count * chain_len, -1)
    groups = gated_rows.reshape(gated_rows.shape[0], N_TP, -1).transpose(1, 0, 2)
    weight_groups = output_weight.reshape(N_TP, -1, D)

    def add_group(running_sum, group_pair):
        group_sum = lax.optimization_barrier(jnp.dot(group_pair[0], group_pair[1], preferred_element_type=jnp.float32).astype(jnp.bfloat16))
        return (running_sum + group_sum.astype(jnp.float32), None)
    running_sum, ignored = lax.scan(add_group, jnp.zeros((gated_rows.shape[0], D), jnp.float32), (groups, weight_groups))
    mixed = running_sum.astype(jnp.bfloat16)
    return (mixed, memory_out, normaliser_out, stable_out, key_b, value_b)
```

```python
import jax
import jax.numpy as jnp
from jax import lax
from jax.experimental import pallas as pl
from jax.experimental.pallas import tpu as pltpu
from jax.sharding import Mesh
from jax.sharding import PartitionSpec as P

D = 4096
DK = 256
NZ, NX, NY, NC = 8, 4, 4, 2
NJ = NY * NC
ROWS = 32
EPS = 1e-06
MESH = pl.DeviceIdType.MESH
F32 = jnp.float32
BF16 = jnp.bfloat16


def log_sigmoid(v):
    return jnp.minimum(v, 0.0) - jnp.log1p(jnp.exp(-jnp.abs(v)))


def nt(a, b):
    return lax.dot_general(a, b, (((1,), (1,)), ((), ())), preferred_element_type=F32)


def tn(a, b):
    return lax.dot_general(a, b, (((0,), (0,)), ((), ())), preferred_element_type=F32)


def split(v):
    high = v.astype(BF16)
    return high, (v - high.astype(F32)).astype(BF16)


def catch_up_kernel(
    mem_ref, norm_ref, stab_ref, pk_ref, pv_ref, pin_ref, pf_ref, acc_ref,
    mem_out, norm_out, stab_out, mem16_out, norm8_out, coef,
):
    s = pl.program_id(0)

    @pl.when(s == 0)
    def _():
        taken = acc_ref[...]
        stab = stab_ref[...]
        logs, run = [], None
        for j in range(4):
            f = jnp.where(j < taken, log_sigmoid(pf_ref[j]), 0.0)
            run = f if run is None else run + f
            logs.append(run)
        total = run
        ends = [total - logs[j] + pin_ref[j] for j in range(4)]
        new = total + stab
        for j in range(4):
            new = jnp.where(j < taken, jnp.maximum(new, ends[j]), new)
        stab_out[...] = new
        carry = jnp.exp(total + stab - new)
        for j in range(4):
            w = jnp.where(j < taken, jnp.exp(ends[j] - new), 0.0) * (DK**-0.5)
            for h in range(2):
                coef[4 * h + j : 4 * h + j + 1, :] = w[h : h + 1]
        coef[8:10, :] = carry

    lane = lax.broadcasted_iota(jnp.int32, (16, 8), 1)
    col = jnp.sum(jnp.where(lane == s, coef[...], 0.0), axis=1, keepdims=True)
    for h in range(2):
        cols = slice(h * DK, (h + 1) * DK)
        weighted = pk_ref[0, :, cols].astype(F32) * col[4 * h : 4 * h + 4]
        carry = col[8 + h : 9 + h]
        high, low = split(weighted)
        vals = pv_ref[0, :, cols]
        new = carry * mem_ref[0, h] + (tn(high, vals) + tn(low, vals))
        mem_out[0, h] = new
        mem16_out[0, h] = new.astype(BF16)
        row = carry * norm_ref[0, h : h + 1] + jnp.sum(weighted, axis=0, keepdims=True)
        norm_out[0, h : h + 1] = row
        norm8_out[h, pl.ds(s, 1), :] = row


def catch_up(mem, norm, stab_t, pk, pv, pin_t, pf_t, acc):
    whole = lambda *dims: pl.BlockSpec(dims, lambda s: (0,) * len(dims))
    each = lambda *dims: pl.BlockSpec((1, *dims), lambda s: (s,) + (0,) * len(dims))
    return pl.pallas_call(
        catch_up_kernel,
        grid=(8,),
        in_specs=[
            each(2, DK, DK), each(2, DK), whole(2, 8), each(4, 512), each(4, 512),
            whole(4, 2, 8), whole(4, 2, 8), whole(1, 8),
        ],
        out_specs=[
            each(2, DK, DK), each(2, DK), whole(2, 8), each(2, DK, DK), whole(2, 8, DK),
        ],
        out_shape=[
            jax.ShapeDtypeStruct((8, 2, DK, DK), F32),
            jax.ShapeDtypeStruct((8, 2, DK), F32),
            jax.ShapeDtypeStruct((2, 8), F32),
            jax.ShapeDtypeStruct((8, 2, DK, DK), BF16),
            jax.ShapeDtypeStruct((2, 8, DK), F32),
        ],
        scratch_shapes=[pltpu.VMEM((16, 8), F32)],
        name="catch_up",
    )(mem, norm, stab_t, pk, pv, pin_t, pf_t, acc)


def step_kernel(
    tok_ref, gain_ref, wq_ref, wk_ref, wv_ref, wg_ref, gin_ref, gf_ref, bias_ref, wo_ref,
    mem_ref, norm_ref, stab_ref,
    mixed_ref, keys_ref, values_ref,
    wbuf, wob, tok_own, tokbuf, tg, pbuf, rbuf, sbuf, srecv, memv, gin_v, gf_v, gbuf, ebuf, obuf,
    loc_sem, xs_sem, xr_sem, ts_sem, tr_sem, rs_sem, rr_sem, ss_sem, sr_sem, gs_sem, gr_sem,
    es_sem, er_sem,
):
    z, x = lax.axis_index("z"), lax.axis_index("x")
    y, c = lax.axis_index("y"), lax.axis_index("c")
    j = y * NC + c
    right, left = lax.rem(x + 1, NX), lax.rem(x + NX - 1, NX)
    opposite = lax.rem(x + 2, NX)
    zs = [lax.rem(z + d, NZ) for d in range(NZ)]
    js = [lax.rem(j + d, NJ) for d in range(NJ)]
    self_tok = j == z

    def at_x(other):
        return (z, other, y, c)

    def at_z(other):
        return (other, x, y, c)

    def at_zj(other, tp):
        return (other, x, lax.div(tp, NC), lax.rem(tp, NC))

    def rdma(src, dst, ssem, rsem, dev):
        return pltpu.make_async_remote_copy(
            src_ref=src, dst_ref=dst, send_sem=ssem, recv_sem=rsem,
            device_id=dev, device_id_type=MESH,
        )

    def wblock(p, owner, start, size):
        if p < 4:
            first = pl.multiple_of(owner * 128 + start * 128 // 4, 32)
            return wbuf.at[p, pl.ds(first, size * 128 // 4), :]
        cols = pl.ds(pl.multiple_of(owner * 128, 128), 128)
        return wob.at[pl.ds(start * 128, size * 128), cols]

    weights = (wq_ref, wk_ref, wv_ref, wg_ref, wo_ref)
    local = [pltpu.make_async_copy(weights[p], wblock(p, x, 0, 4), loc_sem.at[p]) for p in range(5)]
    local.append(pltpu.make_async_copy(tok_ref, tok_own, loc_sem.at[5]))
    feats = pl.ds(pl.multiple_of(z * 512, 512), 512)
    local.append(pltpu.make_async_copy(gin_ref.at[:, feats], gin_v, loc_sem.at[6]))
    local.append(pltpu.make_async_copy(gf_ref.at[:, feats], gf_v, loc_sem.at[7]))
    local.append(pltpu.make_async_copy(mem_ref, memv, loc_sem.at[8]))
    for copy in local:
        copy.start()

    barrier = pltpu.get_barrier_semaphore()

    def greet(dev):
        pl.semaphore_signal(barrier, inc=1, device_id=dev, device_id_type=MESH)

    greet(at_x(right))
    greet(at_x(left))
    for d in range(1, NZ):
        greet(at_z(zs[d]))
    for d in range(1, NJ):
        greet(at_zj(j, js[d]))
        greet(at_zj(zs[d], z))

    @pl.when(jnp.logical_not(self_tok))
    def _():
        greet(at_zj(j, j))
        greet(at_zj(z, z))

    pl.semaphore_wait(barrier, jnp.where(self_tok, 23, 25))

    def direct(p):
        return [
            rdma(wblock(p, x, 0, 4), wblock(p, x, 0, 4), xs_sem.at[p, 0], xr_sem.at[p, 0], at_x(right)),
            rdma(wblock(p, x, 0, 4), wblock(p, x, 0, 4), xs_sem.at[p, 1], xr_sem.at[p, 1], at_x(left)),
        ]

    def onward(p):
        return [
            rdma(wblock(p, left, 0, 2), wblock(p, left, 0, 2), xs_sem.at[p, 2], xr_sem.at[p, 2], at_x(right)),
            rdma(wblock(p, right, 2, 2), wblock(p, right, 2, 2), xs_sem.at[p, 3], xr_sem.at[p, 3], at_x(left)),
        ]

    def arrive(p, which):
        owner, start, size = ((left, 0, 4), (right, 0, 4), (opposite, 0, 2), (opposite, 2, 2))[which]
        block = wblock(p, owner, start, size)
        rdma(block, block, xs_sem.at[p, which], xr_sem.at[p, which], at_x(left)).wait_recv()

    sent = []

    def go(copies):
        for copy in copies:
            copy.start()
            sent.append(copy)

    local[0].wait()
    go(direct(0))
    local[5].wait()
    tok_copies = [
        rdma(tok_own, tokbuf.at[z], ts_sem.at[d], tr_sem.at[z], at_zj(j, js[d])) for d in range(NJ)
    ]
    go(tok_copies[1:])

    @pl.when(jnp.logical_not(self_tok))
    def _():
        tok_copies[0].start()

    @pl.when(self_tok)
    def _():
        tokbuf[z] = tok_own[...]

    local[1].wait()
    go(direct(1))
    local[2].wait()
    local[3].wait()
    local[4].wait()

    row8 = lax.broadcasted_iota(jnp.int32, (8, 16), 0)
    lane16 = lax.broadcasted_iota(jnp.int32, (8, 16), 1)
    pick_in = jnp.where((row8 < 2) & (lane16 == 2 * j + row8), 1.0, 0.0).astype(BF16)
    pick_f = jnp.where((row8 >= 2) & (row8 < 4) & (lane16 == 2 * j + row8 - 2), 1.0, 0.0).astype(BF16)
    local[6].wait()
    local[7].wait()
    gates8 = (
        jnp.dot(pick_in, gin_v[...], preferred_element_type=F32)
        + jnp.dot(pick_f, gf_v[...], preferred_element_type=F32)
    ).astype(BF16)
    ones8 = jnp.full((8, 512), 1.0, BF16)
    row32 = lax.broadcasted_iota(jnp.int32, (8, ROWS), 0)
    gains = jnp.concatenate([gain_ref[pl.ds(4 * z + r, 1), :] for r in range(4)], axis=1)
    sbuf[...] = jnp.zeros_like(sbuf)

    def token_block(d):
        slot = zs[d]
        if d:
            tok_wait = rdma(tok_own, tokbuf.at[slot], ts_sem.at[d], tr_sem.at[slot], at_zj(slot, z))
            tok_wait.wait_recv()
        else:
            @pl.when(jnp.logical_not(self_tok))
            def _():
                rdma(tok_own, tokbuf.at[slot], ts_sem.at[d], tr_sem.at[slot], at_zj(slot, z)).wait_recv()
        raw = tokbuf[slot].astype(F32)
        scaled = (raw * gains).astype(BF16)
        tg[pl.ds(pl.multiple_of(slot * ROWS, ROWS), ROWS), :] = scaled
        high, low = split(raw * raw)
        squares = nt(ones8, high) + nt(ones8, low)
        sbuf[slot, :, 0:ROWS] = jnp.where(row32 == 4, squares, nt(gates8, scaled))

    for d in (0, 1, 7, 2, 6, 3, 5, 4):
        token_block(d)
    far_first = (4, 3, 5, 2, 6, 1, 7)
    small = [rdma(sbuf.at[zs[d]], srecv.at[d], ss_sem.at[d], sr_sem.at[d], at_z(zs[d])) for d in far_first]
    go(small)

    def project(p):
        part = jnp.dot(tg[...], wbuf[p], preferred_element_type=F32)
        pbuf[p] = part.astype(BF16).reshape(NZ, ROWS, 512)
        go([
            rdma(pbuf.at[p, zs[d]], rbuf.at[p, d], rs_sem.at[p, d], rr_sem.at[p, d], at_z(zs[d]))
            for d in far_first
        ])

    def collect(p):
        total = pbuf[p, z].astype(F32)
        for d in range(1, NZ):
            rdma(pbuf.at[p, zs[d]], rbuf.at[p, d], rs_sem.at[p, d], rr_sem.at[p, d], at_z(zs[d])).wait_recv()
            total = total + rbuf[p, d].astype(F32)
        return total

    for p in range(5):
        arrive(p, 0)
        arrive(p, 1)
        go(onward(p))
        if p + 2 < 5:
            go(direct(p + 2))
        if p >= 1:
            arrive(p - 1, 2)
            arrive(p - 1, 3)
            project(p - 1)

    for copy in small:
        copy.wait_recv()
    sums = sbuf[z]
    for d in range(1, NZ):
        sums = sums + srecv[d]
    scale_row = lax.rsqrt(sums[4:5, 0:ROWS] / D + EPS)
    ri = lax.broadcasted_iota(jnp.int32, (ROWS, ROWS), 0)
    ci = lax.broadcasted_iota(jnp.int32, (ROWS, ROWS), 1)
    eye = ri == ci
    same = lax.div(ri, 4) == lax.div(ci, 4)
    causal = same & (ci <= ri)
    anti = same & (ri <= ci)

    def to_col(row):
        return jnp.sum(jnp.where(eye, row, 0.0), axis=1, keepdims=True)

    scale_col = to_col(scale_row)
    seq_of_row = lax.div(lax.broadcasted_iota(jnp.int32, (ROWS, 8), 0), 4)
    seq_lane = lax.broadcasted_iota(jnp.int32, (ROWS, 8), 1)
    own_seq = seq_of_row == seq_lane
    row_seq = lax.div(lax.broadcasted_iota(jnp.int32, (ROWS, DK), 0), 4)

    local[8].wait()
    query = (collect(0) * scale_col).astype(BF16)
    carried_rows = []
    for h in range(2):
        q = query[:, h * DK : (h + 1) * DK]
        read = jnp.zeros((ROWS, DK), F32)
        for s in range(8):
            part = jnp.dot(q, memv[s, h], preferred_element_type=F32)
            read = jnp.where(row_seq == s, part, read)
        carried_rows.append(read)
    key = (collect(1) * scale_col).astype(BF16)
    keys_ref[...] = key
    value = (collect(2) * scale_col).astype(BF16)
    values_ref[...] = value

    hidden = []
    for h in range(2):
        cols = slice(h * DK, (h + 1) * DK)
        q, k, v = query[:, cols], key[:, cols], value[:, cols]
        in_row = sums[h : h + 1, 0:ROWS] * scale_row
        f_row = log_sigmoid(sums[2 + h : 3 + h, 0:ROWS] * scale_row + bias_ref[2 * j + h])
        f_col = to_col(f_row)
        b_col = jnp.sum(jnp.where(causal, f_row, 0.0), axis=1, keepdims=True)
        b_row = jnp.sum(jnp.where(anti, f_col, 0.0), axis=0, keepdims=True)
        within = jnp.where(causal, b_col - b_row + in_row, -jnp.inf)
        stab_col = jnp.sum(jnp.where(own_seq, stab_ref[h : h + 1, :], 0.0), axis=1, keepdims=True)
        g_col = b_col + stab_col
        level = jnp.maximum(g_col, jnp.max(within, axis=1, keepdims=True))
        u = jnp.exp(g_col - level)
        w = nt(q, k) * (DK**-0.5) * jnp.where(causal, jnp.exp(within - level), 0.0)
        w_high, w_low = split(w)
        n_high, n_low = split(norm_ref[h])
        q_norm = jnp.sum(jnp.where(own_seq, nt(q, n_high) + nt(q, n_low), 0.0), axis=1, keepdims=True)
        num = u * carried_rows[h] + (
            jnp.dot(w_high, v, preferred_element_type=F32) + jnp.dot(w_low, v, preferred_element_type=F32)
        )
        den = u * q_norm + jnp.sum(w, axis=1, keepdims=True)
        hidden.append(num / jnp.maximum(jnp.abs(den), 1.0))

    arrive(4, 2)
    arrive(4, 3)

    gate = jax.nn.sigmoid((collect(3) * scale_col).astype(BF16).astype(F32))
    gbuf[z] = (gate * jnp.concatenate(hidden, axis=1)).astype(BF16)
    go([
        rdma(gbuf.at[z], gbuf.at[z], gs_sem.at[d], gr_sem.at[d], at_z(zs[d])) for d in far_first
    ])

    for d in (0, 1, 7, 2, 6, 3, 5, 4):
        slot = zs[d]
        if d:
            came = NZ - d
            rdma(gbuf.at[slot], gbuf.at[slot], gs_sem.at[came], gr_sem.at[came], at_z(slot)).wait_recv()
        ebuf[slot] = jnp.dot(gbuf[slot], wob[...], preferred_element_type=F32).astype(BF16)
        out = rdma(ebuf.at[slot], obuf.at[j], es_sem.at[d], er_sem.at[j], at_zj(slot, z))
        if d:
            go([out])
        else:
            own_out = out

            @pl.when(jnp.logical_not(self_tok))
            def _():
                own_out.start()

            @pl.when(self_tok)
            def _():
                obuf[j] = ebuf[slot]

    total = None
    for d in range(NJ):
        slot = js[d]
        if d:
            rdma(ebuf.at[0], obuf.at[slot], es_sem.at[d], er_sem.at[slot], at_zj(j, slot)).wait_recv()
        else:
            @pl.when(jnp.logical_not(self_tok))
            def _():
                rdma(ebuf.at[0], obuf.at[slot], es_sem.at[d], er_sem.at[slot], at_zj(j, slot)).wait_recv()
        term = obuf[slot].astype(F32)
        total = term if total is None else total + term
    mixed_ref[...] = total.astype(BF16)

    for copy in sent:
        copy.wait_send()

    @pl.when(jnp.logical_not(self_tok))
    def _():
        tok_copies[0].wait_send()
        own_out.wait_send()


def step(tok, gain, wq, wk, wv, wg, gin_t, gf_t, bias, wo, mem16, norm8, stab_t):
    hbm = pl.BlockSpec(memory_space=pl.ANY)
    vmem = pl.BlockSpec(memory_space=pltpu.VMEM)
    smem = pl.BlockSpec(memory_space=pltpu.SMEM)
    dma = pltpu.SemaphoreType.DMA
    block = lambda *lead: pltpu.VMEM((*lead, ROWS, 512), BF16)
    return pl.pallas_call(
        step_kernel,
        in_specs=[hbm, vmem, hbm, hbm, hbm, hbm, hbm, hbm, smem, hbm, hbm, vmem, vmem],
        out_specs=[vmem, vmem, vmem],
        out_shape=[jax.ShapeDtypeStruct((ROWS, 512), BF16)] * 3,
        scratch_shapes=[
            pltpu.VMEM((4, 512, 512), BF16),
            pltpu.VMEM((512, 512), BF16),
            block(),
            block(NZ),
            pltpu.VMEM((256, 512), BF16),
            block(4, NZ),
            block(4, NZ),
            pltpu.VMEM((NZ, 8, 128), F32),
            pltpu.VMEM((NZ, 8, 128), F32),
            pltpu.VMEM((8, 2, DK, DK), BF16),
            pltpu.VMEM((16, 512), BF16),
            pltpu.VMEM((16, 512), BF16),
            block(NZ),
            block(NZ),
            block(NJ),
            dma((9,)), dma((5, 4)), dma((5, 4)), dma((8,)), dma((8,)), dma((4, 8)), dma((4, 8)),
            dma((8,)), dma((8,)), dma((8,)), dma((8,)), dma((8,)), dma((8,)),
        ],
        compiler_params=pltpu.CompilerParams(
            collective_id=0, has_side_effects=True, vmem_limit_bytes=40 * 1024 * 1024
        ),
        name="step",
    )(tok, gain, wq, wk, wv, wg, gin_t, gf_t, bias, wo, mem16, norm8, stab_t)


def body(
    tokens, norm_gain, query_weight, key_weight, value_weight, outgate_weight, ingate_weight,
    forget_weight, forget_bias, output_weight, state_memory, state_normaliser, state_stabiliser,
    past_keys, past_values, past_ingate, past_forget, accepted,
):
    memory, normaliser, stab_t, mem16, norm8 = catch_up(
        state_memory, state_normaliser, state_stabiliser.T, past_keys, past_values,
        past_ingate.transpose(1, 2, 0), past_forget.transpose(1, 2, 0), accepted.reshape(1, 8),
    )
    mixed, keys, values = step(
        tokens, norm_gain.reshape(32, 128), query_weight, key_weight, value_weight, outgate_weight,
        ingate_weight.T, forget_weight.T, forget_bias, output_weight, mem16, norm8, stab_t,
    )
    return (mixed, memory, normaliser, stab_t.T, keys, values)


def solution(mesh):
    torus = Mesh(mesh.devices.reshape(NZ, NX, NY, NC), ("z", "x", "y", "c"))
    kv, tp = ("z", "x"), ("y", "c")
    in_specs = (
        P(kv, tp), P(), P(kv, tp), P(kv, tp), P(kv, tp), P(kv, tp), P(), P(), P(), P(tp, kv),
        P(kv, tp, None, None), P(kv, tp, None), P(kv, tp), P(kv, None, tp), P(kv, None, tp),
        P(kv, None, tp), P(kv, None, tp), P(kv),
    )
    out_specs = (
        P(kv, tp), P(kv, tp, None, None), P(kv, tp, None), P(kv, tp), P(kv, tp), P(kv, tp),
    )
    return jax.shard_map(body, mesh=torus, in_specs=in_specs, out_specs=out_specs, check_vma=False)
```

```python
import jax
import jax.numpy as jnp
from jax import lax
from jax.experimental import pallas as pl
from jax.experimental.pallas import tpu as pltpu
from jax.sharding import Mesh
from jax.sharding import PartitionSpec as P

D = 4096
DK = 256
NZ, NX, NY, NC = 8, 4, 4, 2
NJ = NY * NC
ROWS = 32
EPS = 1e-06
MESH = pl.DeviceIdType.MESH
F32 = jnp.float32
BF16 = jnp.bfloat16


def log_sigmoid(v):
    return jnp.minimum(v, 0.0) - jnp.log1p(jnp.exp(-jnp.abs(v)))


def nt(a, b):
    return lax.dot_general(a, b, (((1,), (1,)), ((), ())), preferred_element_type=F32)


def tn(a, b):
    return lax.dot_general(a, b, (((0,), (0,)), ((), ())), preferred_element_type=F32)


def split(v):
    high = v.astype(BF16)
    return high, (v - high.astype(F32)).astype(BF16)


def step_kernel(
    tok_ref, gain_ref, wq_ref, wk_ref, wv_ref, wg_ref, gin_ref, gf_ref, bias_ref, wo_ref,
    mem_ref, norm_ref, stab_ref, pk_ref, pv_ref, pin_ref, pf_ref, acc_ref,
    terms_ref, mem_out, norm_out, stab_out, keys_ref, values_ref,
    wbuf, wob, tok_own, tok_mid, tokbuf, tg, pbuf, rbuf, sbuf, srecv, memv, gin_v, gf_v, gbuf, ebuf,
    gain_v, norm_v, stab_v, pk_v, pv_v, pin_v, pf_v, acc_v, bias_v, coef, norm8,
    loc_sem, xs_sem, xr_sem, ys_sem, yr_sem, ts_sem, tr_sem, rs_sem, rr_sem, ss_sem, sr_sem,
    gs_sem, gr_sem, es_sem, er_sem,
):
    z, x = lax.axis_index("z"), lax.axis_index("x")
    y, c = lax.axis_index("y"), lax.axis_index("c")
    j = y * NC + c
    right, left = lax.rem(x + 1, NX), lax.rem(x + NX - 1, NX)
    opposite = lax.rem(x + 2, NX)
    zs = [lax.rem(z + d, NZ) for d in range(NZ)]
    js = [lax.rem(j + d, NJ) for d in range(NJ)]
    ys = [lax.rem(y + d, NY) for d in range(NY)]
    self_tok = j == z

    def at_x(other):
        return (z, other, y, c)

    def at_z(other):
        return (other, x, y, c)

    def at_y(other):
        return (z, x, other, c)

    def at_zj(other, tp):
        return (other, x, lax.div(tp, NC), lax.rem(tp, NC))

    def rdma(src, dst, ssem, rsem, dev):
        return pltpu.make_async_remote_copy(
            src_ref=src, dst_ref=dst, send_sem=ssem, recv_sem=rsem,
            device_id=dev, device_id_type=MESH,
        )

    def wblock(p, owner, start, size):
        if p < 4:
            first = pl.multiple_of(owner * 128 + start * 32, 32)
            return wbuf.at[p, pl.ds(first, size * 32), :]
        cols = pl.ds(pl.multiple_of(owner * 128, 128), 128)
        return wob.at[pl.ds(start * 128, size * 128), cols]

    feats = pl.ds(pl.multiple_of(z * 512, 512), 512)
    moves = (
        (wq_ref, wblock(0, x, 0, 4)), (wk_ref, wblock(1, x, 0, 4)), (wv_ref, wblock(2, x, 0, 4)),
        (wg_ref, wblock(3, x, 0, 4)), (wo_ref, wblock(4, x, 0, 4)), (tok_ref, tok_own),
        (gin_ref.at[:, feats], gin_v), (gf_ref.at[:, feats], gf_v), (mem_ref, mem_out),
        (gain_ref, gain_v), (norm_ref, norm_v), (stab_ref, stab_v), (pk_ref, pk_v), (pv_ref, pv_v),
        (pin_ref, pin_v), (pf_ref, pf_v), (acc_ref, acc_v), (bias_ref, bias_v),
    )
    local = [pltpu.make_async_copy(src, dst, loc_sem.at[i]) for i, (src, dst) in enumerate(moves)]
    for i in (0, 5, 1, 2, 3, 4, 6, 7, 9, 10, 11, 12, 13, 14, 15, 16, 17, 8):
        local[i].start()

    barrier = pltpu.get_barrier_semaphore()

    def greet(dev):
        pl.semaphore_signal(barrier, inc=1, device_id=dev, device_id_type=MESH)

    greet(at_x(right))
    greet(at_x(left))
    for d in range(1, NZ):
        greet(at_z(zs[d]))
        greet((zs[d], x, y, 1 - c))
    for d in range(1, NJ):
        greet(at_zj(z, js[d]))
    pl.semaphore_wait(barrier, 23)

    def direct(p):
        return [
            rdma(wblock(p, x, 0, 4), wblock(p, x, 0, 4), xs_sem.at[p, 0], xr_sem.at[p, 0], at_x(right)),
            rdma(wblock(p, x, 0, 4), wblock(p, x, 0, 4), xs_sem.at[p, 1], xr_sem.at[p, 1], at_x(left)),
        ]

    def onward(p):
        return [
            rdma(wblock(p, left, 0, 2), wblock(p, left, 0, 2), xs_sem.at[p, 2], xr_sem.at[p, 2], at_x(right)),
            rdma(wblock(p, right, 2, 2), wblock(p, right, 2, 2), xs_sem.at[p, 3], xr_sem.at[p, 3], at_x(left)),
        ]

    def arrive(p, which):
        owner, start, size = ((left, 0, 4), (right, 0, 4), (opposite, 0, 2), (opposite, 2, 2))[which]
        block = wblock(p, owner, start, size)
        rdma(block, block, xs_sem.at[p, which], xr_sem.at[p, which], at_x(left)).wait_recv()

    sent = []

    def go(copies):
        for copy in copies:
            copy.start()
            sent.append(copy)

    local[0].wait()
    go(direct(0))
    local[5].wait()
    go([rdma(tok_own, tok_mid.at[y], ys_sem.at[d], yr_sem.at[y], at_y(ys[d])) for d in (2, 1, 3)])
    local[1].wait()
    go(direct(1))

    for i in (11, 14, 15, 16):
        local[i].wait()
    taken = acc_v[...]
    stab = stab_v[...]
    logs, run = [], None
    for i in range(4):
        f = jnp.where(i < taken, log_sigmoid(pf_v[i]), 0.0)
        run = f if run is None else run + f
        logs.append(run)
    ends = [run - logs[i] + pin_v[i] for i in range(4)]
    stab_new = run + stab
    for i in range(4):
        stab_new = jnp.where(i < taken, jnp.maximum(stab_new, ends[i]), stab_new)
    stab_out[...] = stab_new
    for i in range(4):
        w = jnp.where(i < taken, jnp.exp(ends[i] - stab_new), 0.0) * (DK**-0.5)
        for h in range(2):
            coef[4 * h + i : 4 * h + i + 1, :] = w[h : h + 1]
    coef[8:10, :] = jnp.exp(run + stab - stab_new)
    coef[10:16, :] = jnp.zeros((6, 8), F32)
    coef_lane = lax.broadcasted_iota(jnp.int32, (16, 8), 1)
    for i in (8, 10, 12, 13):
        local[i].wait()

    def update(s, carry_in):
        col = jnp.sum(jnp.where(coef_lane == s, coef[...], 0.0), axis=1, keepdims=True)
        for h in range(2):
            cols = slice(h * DK, (h + 1) * DK)
            weighted = pk_v[s, :, cols].astype(F32) * col[4 * h : 4 * h + 4]
            carry = col[8 + h : 9 + h]
            high, low = split(weighted)
            vals = pv_v[s, :, cols]
            new = carry * mem_out[s, h] + (tn(high, vals) + tn(low, vals))
            mem_out[s, h] = new
            memv[s, h] = new.astype(BF16)
            row = carry * norm_v[s, h : h + 1] + jnp.sum(weighted, axis=0, keepdims=True)
            norm_out[s, h : h + 1] = row
            norm8[h, pl.ds(s, 1), :] = row
        return carry_in

    lax.fori_loop(0, 3, update, 0)

    relay_tok = []
    for d in (0, 1, 3, 2):
        far = ys[d] * NC + c
        block = tok_own if d == 0 else tok_mid.at[ys[d]]
        if d:
            rdma(tok_own, block, ys_sem.at[d], yr_sem.at[ys[d]], at_y(ys[d])).wait_recv()
        for core in range(NC):
            copy = rdma(
                block, tokbuf.at[z], ts_sem.at[2 * d + core], tr_sem.at[z],
                (far, x, y, lax.rem(c + core, NC)),
            )
            relay_tok.append((copy, far))

            @pl.when(jnp.logical_not((far == z) & (core == 0)))
            def _(copy=copy):
                copy.start()

        @pl.when(far == z)
        def _(block=block):
            tokbuf[z] = block[...]

    lax.fori_loop(3, 8, update, 0)
    local[2].wait()
    local[3].wait()
    local[4].wait()

    row8 = lax.broadcasted_iota(jnp.int32, (8, 16), 0)
    lane16 = lax.broadcasted_iota(jnp.int32, (8, 16), 1)
    pick_in = jnp.where((row8 < 2) & (lane16 == 2 * j + row8), 1.0, 0.0).astype(BF16)
    pick_f = jnp.where((row8 >= 2) & (row8 < 4) & (lane16 == 2 * j + row8 - 2), 1.0, 0.0).astype(BF16)
    local[6].wait()
    local[7].wait()
    gates8 = (
        jnp.dot(pick_in, gin_v[...], preferred_element_type=F32)
        + jnp.dot(pick_f, gf_v[...], preferred_element_type=F32)
    ).astype(BF16)
    ones8 = jnp.full((8, 512), 1.0, BF16)
    row32 = lax.broadcasted_iota(jnp.int32, (8, ROWS), 0)
    local[9].wait()
    gains = jnp.concatenate([gain_v[pl.ds(4 * z + r, 1), :] for r in range(4)], axis=1)
    sbuf[...] = jnp.zeros_like(sbuf)

    def token_block(d):
        slot = zs[d]
        landed = rdma(tok_own, tokbuf.at[slot], ts_sem.at[d], tr_sem.at[slot], at_z(zs[1]))
        if d:
            landed.wait_recv()
        else:
            @pl.when(lax.rem(z, NC) != c)
            def _():
                landed.wait_recv()
        raw = tokbuf[slot].astype(F32)
        scaled = (raw * gains).astype(BF16)
        tg[pl.ds(pl.multiple_of(slot * ROWS, ROWS), ROWS), :] = scaled
        high, low = split(raw * raw)
        squares = nt(ones8, high) + nt(ones8, low)
        sbuf[slot, :, 0:ROWS] = jnp.where(row32 == 4, squares, nt(gates8, scaled))

    for d in (0, 1, 7, 2, 6, 3, 5, 4):
        token_block(d)
    far_first = (4, 3, 5, 2, 6, 1, 7)
    small = [rdma(sbuf.at[zs[d]], srecv.at[d], ss_sem.at[d], sr_sem.at[d], at_z(zs[d])) for d in far_first]
    go(small)

    def hop(p, block, slot, to):
        return rdma(block, rbuf.at[p, slot], rs_sem.at[p, slot], rr_sem.at[p, slot], at_z(zs[to]))

    def landed(p, slot):
        hop(p, pbuf.at[p, z], slot, 1).wait_recv()
        return rbuf[p, slot].astype(F32)

    def project(p):
        part = jnp.dot(tg[...], wbuf[p], preferred_element_type=F32)
        pbuf[p] = part.astype(BF16).reshape(NZ, ROWS, 512)
        go([
            hop(p, pbuf.at[p, zs[4]], 4, 2 if p % 2 else 6),
            hop(p, pbuf.at[p, zs[3]], 3, 1),
            hop(p, pbuf.at[p, zs[5]], 5, 7),
            hop(p, pbuf.at[p, zs[1]], 1, 1),
            hop(p, pbuf.at[p, zs[7]], 7, 7),
        ])

    def relay(p):
        for to, near in ((2, 3), (6, 5)):
            total = pbuf[p, zs[to]].astype(F32) + landed(p, near)
            if (p % 2 == 0) == (to == 6):
                total = total + landed(p, 4)
            pbuf[p, zs[to]] = total.astype(BF16)
            go([hop(p, pbuf.at[p, zs[to]], to, to)])

    def collect(p):
        total = pbuf[p, z].astype(F32)
        for slot in (1, 7, 2, 6):
            total = total + landed(p, slot)
        return total

    for p in range(4):
        arrive(p, 0)
        arrive(p, 1)
        go(onward(p))
        if p < 2:
            go(direct(p + 2))
        if p == 3:
            go(direct(4))
        if p >= 1:
            arrive(p - 1, 2)
            arrive(p - 1, 3)
            project(p - 1)
        if p >= 2:
            relay(p - 2)
    arrive(3, 2)
    arrive(3, 3)
    project(3)
    relay(2)
    arrive(4, 0)
    arrive(4, 1)
    go(onward(4))

    for copy in small:
        copy.wait_recv()
    sums = sbuf[z]
    for d in range(1, NZ):
        sums = sums + srecv[d]
    scale_row = lax.rsqrt(sums[4:5, 0:ROWS] / D + EPS)
    ri = lax.broadcasted_iota(jnp.int32, (ROWS, ROWS), 0)
    ci = lax.broadcasted_iota(jnp.int32, (ROWS, ROWS), 1)
    eye = ri == ci
    same = lax.div(ri, 4) == lax.div(ci, 4)
    causal = same & (ci <= ri)
    anti = same & (ri <= ci)

    def to_col(row):
        return jnp.sum(jnp.where(eye, row, 0.0), axis=1, keepdims=True)

    scale_col = to_col(scale_row)
    seq_of_row = lax.div(lax.broadcasted_iota(jnp.int32, (ROWS, 8), 0), 4)
    seq_lane = lax.broadcasted_iota(jnp.int32, (ROWS, 8), 1)
    own_seq = seq_of_row == seq_lane
    row_seq = lax.div(lax.broadcasted_iota(jnp.int32, (ROWS, DK), 0), 4)

    query = (collect(0) * scale_col).astype(BF16)
    carried_rows = []
    for h in range(2):
        q = query[:, h * DK : (h + 1) * DK]
        read = jnp.zeros((ROWS, DK), F32)
        for s in range(8):
            part = jnp.dot(q, memv[s, h], preferred_element_type=F32)
            read = jnp.where(row_seq == s, part, read)
        carried_rows.append(read)
    key = (collect(1) * scale_col).astype(BF16)
    keys_ref[...] = key
    value = (collect(2) * scale_col).astype(BF16)
    values_ref[...] = value

    local[17].wait()
    bias_lane = lax.broadcasted_iota(jnp.int32, (1, 16), 1)
    hidden = []
    for h in range(2):
        cols = slice(h * DK, (h + 1) * DK)
        q, k, v = query[:, cols], key[:, cols], value[:, cols]
        bias = jnp.sum(jnp.where(bias_lane == 2 * j + h, bias_v[...], 0.0), axis=1, keepdims=True)
        in_row = sums[h : h + 1, 0:ROWS] * scale_row
        f_row = log_sigmoid(sums[2 + h : 3 + h, 0:ROWS] * scale_row + bias)
        f_col = to_col(f_row)
        b_col = jnp.sum(jnp.where(causal, f_row, 0.0), axis=1, keepdims=True)
        b_row = jnp.sum(jnp.where(anti, f_col, 0.0), axis=0, keepdims=True)
        within = jnp.where(causal, b_col - b_row + in_row, -jnp.inf)
        stab_col = jnp.sum(jnp.where(own_seq, stab_out[h : h + 1, :], 0.0), axis=1, keepdims=True)
        g_col = b_col + stab_col
        level = jnp.maximum(g_col, jnp.max(within, axis=1, keepdims=True))
        u = jnp.exp(g_col - level)
        w = nt(q, k) * (DK**-0.5) * jnp.where(causal, jnp.exp(within - level), 0.0)
        w_high, w_low = split(w)
        n_high, n_low = split(norm8[h])
        q_norm = jnp.sum(jnp.where(own_seq, nt(q, n_high) + nt(q, n_low), 0.0), axis=1, keepdims=True)
        num = u * carried_rows[h] + (
            jnp.dot(w_high, v, preferred_element_type=F32) + jnp.dot(w_low, v, preferred_element_type=F32)
        )
        den = u * q_norm + jnp.sum(w, axis=1, keepdims=True)
        hidden.append(num / jnp.maximum(jnp.abs(den), 1.0))

    relay(3)
    arrive(4, 2)
    arrive(4, 3)

    gate = jax.nn.sigmoid((collect(3) * scale_col).astype(BF16).astype(F32))
    gbuf[z] = (gate * jnp.concatenate(hidden, axis=1)).astype(BF16)
    go([
        rdma(gbuf.at[z], gbuf.at[z], gs_sem.at[d], gr_sem.at[d], at_z(zs[d])) for d in far_first
    ])

    for d in (0, 1, 7, 2, 6, 3, 5, 4):
        slot = zs[d]
        if d:
            came = NZ - d
            rdma(gbuf.at[slot], gbuf.at[slot], gs_sem.at[came], gr_sem.at[came], at_z(slot)).wait_recv()
        ebuf[slot] = jnp.dot(gbuf[slot], wob[...], preferred_element_type=F32).astype(BF16)
        out = rdma(ebuf.at[slot], terms_ref.at[j], es_sem.at[d], er_sem.at[j], at_zj(slot, z))
        if d:
            go([out])
        else:
            own_out = out

            @pl.when(jnp.logical_not(self_tok))
            def _():
                own_out.start()

            @pl.when(self_tok)
            def _():
                terms_ref[j] = ebuf[slot]

    for d in range(NJ):
        slot = js[d]
        came = rdma(ebuf.at[0], terms_ref.at[slot], es_sem.at[d], er_sem.at[slot], at_zj(z, slot))
        if d:
            came.wait_recv()
        else:
            @pl.when(jnp.logical_not(self_tok))
            def _(came=came):
                came.wait_recv()

    for copy in sent:
        copy.wait_send()
    for i, (copy, far) in enumerate(relay_tok):
        @pl.when(jnp.logical_not((far == z) & (i % 2 == 0)))
        def _(copy=copy):
            copy.wait_send()

    @pl.when(jnp.logical_not(self_tok))
    def _():
        own_out.wait_send()


def finish_kernel(terms, mem, norm, stab, keys, values, mixed, mem_o, norm_o, stab_o, keys_o, values_o, sem):
    copy = pltpu.make_async_copy(mem, mem_o, sem)
    copy.start()
    norm_o[...] = norm[...]
    stab_o[...] = stab[...]
    keys_o[...] = keys[...]
    values_o[...] = values[...]
    total = terms[0].astype(F32)
    for i in range(1, NJ):
        total = total + terms[i].astype(F32)
    mixed[...] = total.astype(BF16)
    copy.wait()


def step(*args):
    args = [pltpu.with_memory_space_constraint(a, pltpu.HBM) for a in args]
    hbm = pl.BlockSpec(memory_space=pltpu.HBM)
    vmem = pl.BlockSpec(memory_space=pltpu.VMEM)
    dma = pltpu.SemaphoreType.DMA
    block = lambda *lead: pltpu.VMEM((*lead, ROWS, 512), BF16)
    shape = jax.ShapeDtypeStruct
    outs = [
        shape((NJ, ROWS, 512), BF16), shape((8, 2, DK, DK), F32), shape((8, 2, DK), F32),
        shape((2, 8), F32), shape((ROWS, 512), BF16), shape((ROWS, 512), BF16),
    ]
    parts = pl.pallas_call(
        step_kernel,
        in_specs=[hbm] * 18,
        out_specs=[vmem] * 6,
        out_shape=outs,
        scratch_shapes=[
            pltpu.VMEM((4, 512, 512), BF16),
            pltpu.VMEM((512, 512), BF16),
            block(),
            block(NY),
            block(NZ),
            pltpu.VMEM((256, 512), BF16),
            block(4, NZ),
            block(4, NZ),
            pltpu.VMEM((NZ, 8, 128), F32),
            pltpu.VMEM((NZ, 8, 128), F32),
            pltpu.VMEM((8, 2, DK, DK), BF16),
            pltpu.VMEM((16, 512), BF16),
            pltpu.VMEM((16, 512), BF16),
            block(NZ),
            block(NZ),
            pltpu.VMEM((32, 128), F32),
            pltpu.VMEM((8, 2, DK), F32),
            pltpu.VMEM((2, 8), F32),
            pltpu.VMEM((8, 4, 512), BF16),
            pltpu.VMEM((8, 4, 512), BF16),
            pltpu.VMEM((4, 2, 8), F32),
            pltpu.VMEM((4, 2, 8), F32),
            pltpu.VMEM((1, 8), jnp.int32),
            pltpu.VMEM((1, 16), F32),
            pltpu.VMEM((16, 8), F32),
            pltpu.VMEM((2, 8, DK), F32),
            dma((18,)), dma((5, 4)), dma((5, 4)), dma((4,)), dma((4,)), dma((8,)), dma((8,)),
            dma((4, 8)), dma((4, 8)), dma((8,)), dma((8,)), dma((8,)), dma((8,)), dma((8,)), dma((8,)),
        ],
        compiler_params=pltpu.CompilerParams(
            collective_id=0, has_side_effects=True, vmem_limit_bytes=24 * 1024 * 1024
        ),
        name="step",
    )(*args)
    return pl.pallas_call(
        finish_kernel,
        in_specs=[vmem, pl.BlockSpec(memory_space=pl.ANY), vmem, vmem, vmem, vmem],
        out_specs=[vmem, hbm, vmem, vmem, vmem, vmem],
        out_shape=[shape((ROWS, 512), BF16)] + outs[1:],
        scratch_shapes=[dma],
        name="finish",
        compiler_params=pltpu.CompilerParams(vmem_limit_bytes=4 * 1024 * 1024),
    )(*[pltpu.with_memory_space_constraint(part, pltpu.VMEM) for part in parts])


def body(
    tokens, norm_gain, query_weight, key_weight, value_weight, outgate_weight, ingate_weight,
    forget_weight, forget_bias, output_weight, state_memory, state_normaliser, state_stabiliser,
    past_keys, past_values, past_ingate, past_forget, accepted,
):
    mixed, memory, normaliser, stab_t, keys, values = step(
        tokens, norm_gain.reshape(32, 128), query_weight, key_weight, value_weight, outgate_weight,
        ingate_weight.T, forget_weight.T, forget_bias.reshape(1, 16), output_weight,
        state_memory, state_normaliser, state_stabiliser.T, past_keys, past_values,
        past_ingate.transpose(1, 2, 0), past_forget.transpose(1, 2, 0), accepted.reshape(1, 8),
    )
    return (mixed, memory, normaliser, stab_t.T, keys, values)


def solution(mesh):
    torus = Mesh(mesh.devices.reshape(NZ, NX, NY, NC), ("z", "x", "y", "c"))
    kv, tp = ("z", "x"), ("y", "c")
    in_specs = (
        P(kv, tp), P(), P(kv, tp), P(kv, tp), P(kv, tp), P(kv, tp), P(), P(), P(), P(tp, kv),
        P(kv, tp, None, None), P(kv, tp, None), P(kv, tp), P(kv, None, tp), P(kv, None, tp),
        P(kv, None, tp), P(kv, None, tp), P(kv),
    )
    out_specs = (
        P(kv, tp), P(kv, tp, None, None), P(kv, tp, None), P(kv, tp), P(kv, tp), P(kv, tp),
    )
    return jax.shard_map(body, mesh=torus, in_specs=in_specs, out_specs=out_specs, check_vma=False)
```

```python
import jax
import jax.numpy as jnp
from jax import lax
from jax.experimental import pallas as pl
from jax.experimental.pallas import tpu as pltpu
from jax.sharding import Mesh
from jax.sharding import PartitionSpec as P

D = 4096
DK = 256
NZ, NX, NY, NC = 8, 4, 4, 2
NJ = NY * NC
ROWS = 32
EPS = 1e-06
RELAYED = 6
MESH = pl.DeviceIdType.MESH
F32 = jnp.float32
BF16 = jnp.bfloat16


def log_sigmoid(v):
    return jnp.minimum(v, 0.0) - jnp.log1p(jnp.exp(-jnp.abs(v)))


def nt(a, b):
    return lax.dot_general(a, b, (((1,), (1,)), ((), ())), preferred_element_type=F32)


def tn(a, b):
    return lax.dot_general(a, b, (((0,), (0,)), ((), ())), preferred_element_type=F32)


def split(v):
    high = v.astype(BF16)
    return high, (v - high.astype(F32)).astype(BF16)


def step_kernel(
    tok_ref, gain_ref, wq_ref, wk_ref, wv_ref, wg_ref, gin_ref, gf_ref, bias_ref, wo_ref,
    mem_ref, norm_ref, stab_ref, pk_ref, pv_ref, pin_ref, pf_ref, acc_ref,
    terms_ref, mem_out, norm_out, stab_out, keys_ref, values_ref,
    wbuf, wob, tok_own, tok_mid, tokbuf, tg, pbuf, rbuf, sbuf, srecv, memv, gin_v, gf_v, gbuf, ebuf,
    gain_v, norm_v, stab_v, pk_v, pv_v, pin_v, pf_v, acc_v, bias_v, coef, norm8,
    loc_sem, xs_sem, xr_sem, ys_sem, yr_sem, ts_sem, tr_sem, rs_sem, rr_sem, ss_sem, sr_sem,
    gs_sem, gr_sem, es_sem, er_sem,
):
    z, x = lax.axis_index("z"), lax.axis_index("x")
    y, c = lax.axis_index("y"), lax.axis_index("c")
    j = y * NC + c
    right, left = lax.rem(x + 1, NX), lax.rem(x + NX - 1, NX)
    opposite = lax.rem(x + 2, NX)
    zs = [lax.rem(z + d, NZ) for d in range(NZ)]
    js = [lax.rem(j + d, NJ) for d in range(NJ)]
    ys = [lax.rem(y + d, NY) for d in range(NY)]
    self_tok = j == z

    def at_x(other):
        return (z, other, y, c)

    def at_z(other):
        return (other, x, y, c)

    def at_y(other):
        return (z, x, other, c)

    def at_zj(other, tp):
        return (other, x, lax.div(tp, NC), lax.rem(tp, NC))

    def rdma(src, dst, ssem, rsem, dev):
        return pltpu.make_async_remote_copy(
            src_ref=src, dst_ref=dst, send_sem=ssem, recv_sem=rsem,
            device_id=dev, device_id_type=MESH,
        )

    def wblock(p, owner, start, size):
        if p < 8:
            first = pl.multiple_of(owner * 128 + start * 32, 32)
            return wbuf.at[p, pl.ds(first, size * 32), :]
        cols = pl.ds(pl.multiple_of(owner * 128, 128), 128)
        return wob.at[pl.ds(start * 128, size * 128), cols]

    feats = pl.ds(pl.multiple_of(z * 512, 512), 512)
    moves = (
        *(
            (w.at[:, pl.ds(h * DK, DK)], wblock(2 * i + h, x, 0, 4))
            for i, w in enumerate((wq_ref, wk_ref, wv_ref, wg_ref))
            for h in range(2)
        ),
        (wo_ref, wblock(8, x, 0, 4)), (tok_ref, tok_own), (gin_ref.at[:, feats], gin_v), (gf_ref.at[:, feats], gf_v), (mem_ref, mem_out),
        (gain_ref, gain_v), (norm_ref, norm_v), (stab_ref, stab_v), (pk_ref, pk_v), (pv_ref, pv_v),
        (pin_ref, pin_v), (pf_ref, pf_v), (acc_ref, acc_v), (bias_ref, bias_v),
    )
    local = [pltpu.make_async_copy(src, dst, loc_sem.at[i]) for i, (src, dst) in enumerate(moves)]
    for i in (0, 9, 1, 2, 3, 4, 5, 6, 7, 15, 18, 19, 20, 13, 14, 16, 17, 10, 11, 21, 8, 12):
        local[i].start()

    barrier = pltpu.get_barrier_semaphore()

    def greet(dev):
        pl.semaphore_signal(barrier, inc=1, device_id=dev, device_id_type=MESH)

    greet(at_x(right))
    greet(at_x(left))
    for d in range(1, NZ):
        greet(at_z(zs[d]))
        greet((zs[d], x, y, 1 - c))
    for d in range(1, NJ):
        greet(at_zj(z, js[d]))
    pl.semaphore_wait(barrier, 23)

    def direct(p):
        return [
            rdma(wblock(p, x, 0, 4), wblock(p, x, 0, 4), xs_sem.at[p, 0], xr_sem.at[p, 0], at_x(right)),
            rdma(wblock(p, x, 0, 4), wblock(p, x, 0, 4), xs_sem.at[p, 1], xr_sem.at[p, 1], at_x(left)),
        ]

    def onward(p):
        return [
            rdma(wblock(p, left, 0, 2), wblock(p, left, 0, 2), xs_sem.at[p, 2], xr_sem.at[p, 2], at_x(right)),
            rdma(wblock(p, right, 2, 2), wblock(p, right, 2, 2), xs_sem.at[p, 3], xr_sem.at[p, 3], at_x(left)),
        ]

    def arrive(p, which):
        owner, start, size = ((left, 0, 4), (right, 0, 4), (opposite, 0, 2), (opposite, 2, 2))[which]
        block = wblock(p, owner, start, size)
        rdma(block, block, xs_sem.at[p, which], xr_sem.at[p, which], at_x(left)).wait_recv()

    sent = []

    def go(copies):
        for copy in copies:
            copy.start()
            sent.append(copy)

    def forward(p):
        arrive(p, 0)
        arrive(p, 1)
        go(onward(p))
        if p < 5:
            local[p + 3].wait()
            go(direct(p + 3))

    local[0].wait()
    go(direct(0))
    local[9].wait()
    go([rdma(tok_own, tok_mid.at[y], ys_sem.at[d], yr_sem.at[y], at_y(ys[d])) for d in (2, 1, 3)])
    for p in (1, 2):
        local[p].wait()
        go(direct(p))

    for i in (15, 18, 19, 20):
        local[i].wait()
    taken = acc_v[...]
    stab = stab_v[...]
    logs, run = [], None
    for i in range(4):
        f = jnp.where(i < taken, log_sigmoid(pf_v[i]), 0.0)
        run = f if run is None else run + f
        logs.append(run)
    ends = [run - logs[i] + pin_v[i] for i in range(4)]
    stab_new = run + stab
    for i in range(4):
        stab_new = jnp.where(i < taken, jnp.maximum(stab_new, ends[i]), stab_new)
    stab_out[...] = stab_new
    for i in range(4):
        w = jnp.where(i < taken, jnp.exp(ends[i] - stab_new), 0.0) * (DK**-0.5)
        for h in range(2):
            coef[4 * h + i : 4 * h + i + 1, :] = w[h : h + 1]
    coef[8:10, :] = jnp.exp(run + stab - stab_new)
    coef[10:16, :] = jnp.zeros((6, 8), F32)
    coef_lane = lax.broadcasted_iota(jnp.int32, (16, 8), 1)
    for i in (12, 14, 16, 17):
        local[i].wait()

    def update(s, carry_in):
        col = jnp.sum(jnp.where(coef_lane == s, coef[...], 0.0), axis=1, keepdims=True)
        for h in range(2):
            cols = slice(h * DK, (h + 1) * DK)
            weighted = pk_v[s, :, cols].astype(F32) * col[4 * h : 4 * h + 4]
            carry = col[8 + h : 9 + h]
            high, low = split(weighted)
            vals = pv_v[s, :, cols]
            new = carry * mem_out[s, h] + (tn(high, vals) + tn(low, vals))
            mem_out[s, h] = new
            memv[s, h] = new.astype(BF16)
            row = carry * norm_v[s, h : h + 1] + jnp.sum(weighted, axis=0, keepdims=True)
            norm_out[s, h : h + 1] = row
            norm8[h, pl.ds(s, 1), :] = row
        return carry_in

    forward(0)
    lax.fori_loop(0, 1, update, 0)

    relay_tok = []
    for d in (0, 1, 3, 2):
        far = ys[d] * NC + c
        block = tok_own if d == 0 else tok_mid.at[ys[d]]
        if d:
            rdma(tok_own, block, ys_sem.at[d], yr_sem.at[ys[d]], at_y(ys[d])).wait_recv()
        for core in range(NC):
            copy = rdma(
                block, tokbuf.at[z], ts_sem.at[2 * d + core], tr_sem.at[z],
                (far, x, y, lax.rem(c + core, NC)),
            )
            relay_tok.append((copy, far))

            @pl.when(jnp.logical_not((far == z) & (core == 0)))
            def _(copy=copy):
                copy.start()

        @pl.when(far == z)
        def _(block=block):
            tokbuf[z] = block[...]

    forward(1)
    lax.fori_loop(1, 4, update, 0)
    forward(2)
    lax.fori_loop(4, 8, update, 0)
    forward(3)
    row8 = lax.broadcasted_iota(jnp.int32, (8, 16), 0)
    lane16 = lax.broadcasted_iota(jnp.int32, (8, 16), 1)
    pick_in = jnp.where((row8 < 2) & (lane16 == 2 * j + row8), 1.0, 0.0).astype(BF16)
    pick_f = jnp.where((row8 >= 2) & (row8 < 4) & (lane16 == 2 * j + row8 - 2), 1.0, 0.0).astype(BF16)
    local[10].wait()
    local[11].wait()
    gates8 = (
        jnp.dot(pick_in, gin_v[...], preferred_element_type=F32)
        + jnp.dot(pick_f, gf_v[...], preferred_element_type=F32)
    ).astype(BF16)
    ones8 = jnp.full((8, 512), 1.0, BF16)
    row32 = lax.broadcasted_iota(jnp.int32, (8, ROWS), 0)
    local[13].wait()
    gains = jnp.concatenate([gain_v[pl.ds(4 * z + r, 1), :] for r in range(4)], axis=1)
    sbuf[...] = jnp.zeros_like(sbuf)

    def token_block(d):
        slot = zs[d]
        landed = rdma(tok_own, tokbuf.at[slot], ts_sem.at[d], tr_sem.at[slot], at_z(zs[1]))
        if d:
            landed.wait_recv()
        else:
            @pl.when(lax.rem(z, NC) != c)
            def _():
                landed.wait_recv()
        raw = tokbuf[slot].astype(F32)
        scaled = (raw * gains).astype(BF16)
        tg[pl.ds(pl.multiple_of(slot * ROWS, ROWS), ROWS), :] = scaled
        high, low = split(raw * raw)
        squares = nt(ones8, high) + nt(ones8, low)
        sbuf[slot, :, 0:ROWS] = jnp.where(row32 == 4, squares, nt(gates8, scaled))

    for d in (0, 1, 7, 2, 6, 3, 5, 4):
        token_block(d)
    far_first = (4, 3, 5, 2, 6, 1, 7)
    small = [rdma(sbuf.at[zs[d]], srecv.at[d], ss_sem.at[d], sr_sem.at[d], at_z(zs[d])) for d in far_first]
    go(small)

    def hop(p, block, slot, to):
        return rdma(block, rbuf.at[p, slot], rs_sem.at[p, slot], rr_sem.at[p, slot], at_z(zs[to]))

    def landed(p, slot):
        hop(p, pbuf.at[p, z], slot, 1).wait_recv()
        return rbuf[p, slot].astype(F32)

    def project(p):
        arrive(p, 2)
        arrive(p, 3)
        part = jnp.dot(tg[...], wbuf[p], preferred_element_type=F32)
        pbuf[p] = part.astype(BF16).reshape(NZ, ROWS, DK)
        if p < RELAYED:
            go([
                hop(p, pbuf.at[p, zs[4]], 4, 2 if p % 2 else 6),
                hop(p, pbuf.at[p, zs[3]], 3, 1),
                hop(p, pbuf.at[p, zs[5]], 5, 7),
                hop(p, pbuf.at[p, zs[1]], 1, 1),
                hop(p, pbuf.at[p, zs[7]], 7, 7),
            ])
        else:
            go([hop(p, pbuf.at[p, zs[d]], d, d) for d in far_first])

    def relay(p):
        for to, near in ((2, 3), (6, 5)):
            total = pbuf[p, zs[to]].astype(F32) + landed(p, near)
            if (p % 2 == 0) == (to == 6):
                total = total + landed(p, 4)
            pbuf[p, zs[to]] = total.astype(BF16)
            go([hop(p, pbuf.at[p, zs[to]], to, to)])

    def collect(p):
        total = pbuf[p, z].astype(F32)
        for slot in (1, 7, 2, 6) if p < RELAYED else (1, 7, 2, 6, 3, 5, 4):
            total = total + landed(p, slot)
        return (total * scale_col).astype(BF16)

    for p in range(8):
        if p < 4:
            forward(p + 4)
        if p == 3:
            local[8].wait()
            go(direct(8))
        project(p)
        if 0 <= p - 3 < RELAYED:
            relay(p - 3)
    for p in range(5, RELAYED):
        relay(p)

    for copy in small:
        copy.wait_recv()
    sums = sbuf[z]
    for d in range(1, NZ):
        sums = sums + srecv[d]
    scale_row = lax.rsqrt(sums[4:5, 0:ROWS] / D + EPS)
    ri = lax.broadcasted_iota(jnp.int32, (ROWS, ROWS), 0)
    ci = lax.broadcasted_iota(jnp.int32, (ROWS, ROWS), 1)
    eye = ri == ci
    same = lax.div(ri, 4) == lax.div(ci, 4)
    causal = same & (ci <= ri)
    anti = same & (ri <= ci)

    def to_col(row):
        return jnp.sum(jnp.where(eye, row, 0.0), axis=1, keepdims=True)

    scale_col = to_col(scale_row)
    seq_of_row = lax.div(lax.broadcasted_iota(jnp.int32, (ROWS, 8), 0), 4)
    seq_lane = lax.broadcasted_iota(jnp.int32, (ROWS, 8), 1)
    own_seq = seq_of_row == seq_lane
    row_seq = lax.div(lax.broadcasted_iota(jnp.int32, (ROWS, DK), 0), 4)

    queries, keys, values, carried_rows = [], [], [], []
    for h in range(2):
        q = collect(h)
        queries.append(q)
        read = jnp.zeros((ROWS, DK), F32)
        for s in range(8):
            part = jnp.dot(q, memv[s, h], preferred_element_type=F32)
            read = jnp.where(row_seq == s, part, read)
        carried_rows.append(read)
    for h in range(2):
        keys.append(collect(2 + h))
        keys_ref[:, h * DK : (h + 1) * DK] = keys[h]
    for h in range(2):
        values.append(collect(4 + h))
        values_ref[:, h * DK : (h + 1) * DK] = values[h]

    local[21].wait()
    bias_lane = lax.broadcasted_iota(jnp.int32, (1, 16), 1)
    hidden = []
    for h in range(2):
        q, k, v = queries[h], keys[h], values[h]
        bias = jnp.sum(jnp.where(bias_lane == 2 * j + h, bias_v[...], 0.0), axis=1, keepdims=True)
        in_row = sums[h : h + 1, 0:ROWS] * scale_row
        f_row = log_sigmoid(sums[2 + h : 3 + h, 0:ROWS] * scale_row + bias)
        f_col = to_col(f_row)
        b_col = jnp.sum(jnp.where(causal, f_row, 0.0), axis=1, keepdims=True)
        b_row = jnp.sum(jnp.where(anti, f_col, 0.0), axis=0, keepdims=True)
        within = jnp.where(causal, b_col - b_row + in_row, -jnp.inf)
        stab_col = jnp.sum(jnp.where(own_seq, stab_out[h : h + 1, :], 0.0), axis=1, keepdims=True)
        g_col = b_col + stab_col
        level = jnp.maximum(g_col, jnp.max(within, axis=1, keepdims=True))
        u = jnp.exp(g_col - level)
        w = nt(q, k) * (DK**-0.5) * jnp.where(causal, jnp.exp(within - level), 0.0)
        w_high, w_low = split(w)
        n_high, n_low = split(norm8[h])
        q_norm = jnp.sum(jnp.where(own_seq, nt(q, n_high) + nt(q, n_low), 0.0), axis=1, keepdims=True)
        num = u * carried_rows[h] + (
            jnp.dot(w_high, v, preferred_element_type=F32) + jnp.dot(w_low, v, preferred_element_type=F32)
        )
        den = u * q_norm + jnp.sum(w, axis=1, keepdims=True)
        hidden.append(num / jnp.maximum(jnp.abs(den), 1.0))

    arrive(8, 0)
    arrive(8, 1)
    go(onward(8))
    for h in range(2):
        gate = jax.nn.sigmoid(collect(6 + h).astype(F32))
        gbuf[h, z] = (gate * hidden[h]).astype(BF16)
        go([
            rdma(gbuf.at[h, z], gbuf.at[h, z], gs_sem.at[h, d], gr_sem.at[h, d], at_z(zs[d]))
            for d in far_first
        ])
    arrive(8, 2)
    arrive(8, 3)

    for d in (0, 1, 7, 2, 6, 3, 5, 4):
        slot = zs[d]
        out = jnp.zeros((ROWS, 512), F32)
        for h in range(2):
            if d:
                came = NZ - d
                rdma(
                    gbuf.at[h, slot], gbuf.at[h, slot], gs_sem.at[h, came], gr_sem.at[h, came], at_z(slot)
                ).wait_recv()
            out = out + jnp.dot(gbuf[h, slot], wob[h * DK : (h + 1) * DK, :], preferred_element_type=F32)
        ebuf[slot] = out.astype(BF16)
        out = rdma(ebuf.at[slot], terms_ref.at[j], es_sem.at[d], er_sem.at[j], at_zj(slot, z))
        if d:
            go([out])
        else:
            own_out = out

            @pl.when(jnp.logical_not(self_tok))
            def _():
                own_out.start()

            @pl.when(self_tok)
            def _():
                terms_ref[j] = ebuf[slot]

    for d in range(NJ):
        slot = js[d]
        came = rdma(ebuf.at[0], terms_ref.at[slot], es_sem.at[d], er_sem.at[slot], at_zj(z, slot))
        if d:
            came.wait_recv()
        else:
            @pl.when(jnp.logical_not(self_tok))
            def _(came=came):
                came.wait_recv()

    for copy in sent:
        copy.wait_send()
    for i, (copy, far) in enumerate(relay_tok):
        @pl.when(jnp.logical_not((far == z) & (i % 2 == 0)))
        def _(copy=copy):
            copy.wait_send()

    @pl.when(jnp.logical_not(self_tok))
    def _():
        own_out.wait_send()


def finish_kernel(terms, mem, norm, stab, keys, values, mixed, mem_o, norm_o, stab_o, keys_o, values_o, total_v, sem):
    pairs = ((mem, mem_o), (norm, norm_o), (stab, stab_o), (keys, keys_o), (values, values_o), (total_v, mixed))
    copies = [pltpu.make_async_copy(src, dst, sem.at[i]) for i, (src, dst) in enumerate(pairs)]
    for copy in copies[1:5]:
        copy.start()
    total = terms[0].astype(F32)
    for i in range(1, NJ):
        total = total + terms[i].astype(F32)
    total_v[...] = total.astype(BF16)
    copies[0].start()
    copies[5].start()
    for copy in copies:
        copy.wait()


def step(*args):
    args = [pltpu.with_memory_space_constraint(a, pltpu.HBM) for a in args]
    hbm = pl.BlockSpec(memory_space=pltpu.HBM)
    vmem = pl.BlockSpec(memory_space=pltpu.VMEM)
    dma = pltpu.SemaphoreType.DMA
    block = lambda *lead: pltpu.VMEM((*lead, ROWS, 512), BF16)
    shape = jax.ShapeDtypeStruct
    outs = [
        shape((NJ, ROWS, 512), BF16), shape((8, 2, DK, DK), F32), shape((8, 2, DK), F32),
        shape((2, 8), F32), shape((ROWS, 512), BF16), shape((ROWS, 512), BF16),
    ]
    parts = pl.pallas_call(
        step_kernel,
        in_specs=[hbm] * 18,
        out_specs=[vmem] * 6,
        out_shape=outs,
        scratch_shapes=[
            pltpu.VMEM((8, 512, DK), BF16),
            pltpu.VMEM((512, 512), BF16),
            block(),
            block(NY),
            block(NZ),
            pltpu.VMEM((256, 512), BF16),
            pltpu.VMEM((8, NZ, ROWS, DK), BF16),
            pltpu.VMEM((8, NZ, ROWS, DK), BF16),
            pltpu.VMEM((NZ, 8, 128), F32),
            pltpu.VMEM((NZ, 8, 128), F32),
            pltpu.VMEM((8, 2, DK, DK), BF16),
            pltpu.VMEM((16, 512), BF16),
            pltpu.VMEM((16, 512), BF16),
            pltpu.VMEM((2, NZ, ROWS, DK), BF16),
            block(NZ),
            pltpu.VMEM((32, 128), F32),
            pltpu.VMEM((8, 2, DK), F32),
            pltpu.VMEM((2, 8), F32),
            pltpu.VMEM((8, 4, 512), BF16),
            pltpu.VMEM((8, 4, 512), BF16),
            pltpu.VMEM((4, 2, 8), F32),
            pltpu.VMEM((4, 2, 8), F32),
            pltpu.VMEM((1, 8), jnp.int32),
            pltpu.VMEM((1, 16), F32),
            pltpu.VMEM((16, 8), F32),
            pltpu.VMEM((2, 8, DK), F32),
            dma((22,)), dma((9, 4)), dma((9, 4)), dma((4,)), dma((4,)), dma((8,)), dma((8,)),
            dma((8, 8)), dma((8, 8)), dma((8,)), dma((8,)), dma((2, 8)), dma((2, 8)), dma((8,)), dma((8,)),
        ],
        compiler_params=pltpu.CompilerParams(
            collective_id=0, has_side_effects=True, vmem_limit_bytes=24 * 1024 * 1024
        ),
        name="step",
    )(*args)
    return pl.pallas_call(
        finish_kernel,
        in_specs=[vmem] + [pl.BlockSpec(memory_space=pl.ANY)] * 5,
        out_specs=[hbm] * 6,
        out_shape=[shape((ROWS, 512), BF16)] + outs[1:],
        scratch_shapes=[pltpu.VMEM((ROWS, 512), BF16), dma((6,))],
        name="finish",
        compiler_params=pltpu.CompilerParams(vmem_limit_bytes=4 * 1024 * 1024),
    )(*[pltpu.with_memory_space_constraint(part, pltpu.VMEM) for part in parts])


def body(
    tokens, norm_gain, query_weight, key_weight, value_weight, outgate_weight, ingate_weight,
    forget_weight, forget_bias, output_weight, state_memory, state_normaliser, state_stabiliser,
    past_keys, past_values, past_ingate, past_forget, accepted,
):
    mixed, memory, normaliser, stab_t, keys, values = step(
        tokens, norm_gain.reshape(32, 128), query_weight, key_weight, value_weight, outgate_weight,
        ingate_weight.T, forget_weight.T, forget_bias.reshape(1, 16), output_weight,
        state_memory, state_normaliser, state_stabiliser.T, past_keys, past_values,
        past_ingate.transpose(1, 2, 0), past_forget.transpose(1, 2, 0), accepted.reshape(1, 8),
    )
    return (mixed, memory, normaliser, stab_t.T, keys, values)


def solution(mesh):
    torus = Mesh(mesh.devices.reshape(NZ, NX, NY, NC), ("z", "x", "y", "c"))
    kv, tp = ("z", "x"), ("y", "c")
    in_specs = (
        P(kv, tp), P(), P(kv, tp), P(kv, tp), P(kv, tp), P(kv, tp), P(), P(), P(), P(tp, kv),
        P(kv, tp, None, None), P(kv, tp, None), P(kv, tp), P(kv, None, tp), P(kv, None, tp),
        P(kv, None, tp), P(kv, None, tp), P(kv),
    )
    out_specs = (
        P(kv, tp), P(kv, tp, None, None), P(kv, tp, None), P(kv, tp), P(kv, tp), P(kv, tp),
    )
    return jax.shard_map(body, mesh=torus, in_specs=in_specs, out_specs=out_specs, check_vma=False)
```

```python
import jax
import jax.numpy as jnp
from jax import lax
from jax.experimental import pallas as pl
from jax.experimental.pallas import tpu as pltpu
from jax.sharding import Mesh
from jax.sharding import PartitionSpec as P

D = 4096
DK = 256
NZ, NX, NY, NC = 8, 4, 4, 2
NJ = NY * NC
ROWS = 32
EPS = 1e-06
MODES = (2, 2, 2, 2, 2, 2, 2, 2)
ORDER = "P0 P1 F6 P2 P3 F7 D B0 P4 B1 P5 B2 S P6 B3 P7 B4 B5 B6 B7"
MESH = pl.DeviceIdType.MESH
F32 = jnp.float32
BF16 = jnp.bfloat16


def log_sigmoid(v):
    return jnp.minimum(v, 0.0) - jnp.log1p(jnp.exp(-jnp.abs(v)))


def nt(a, b):
    return lax.dot_general(a, b, (((1,), (1,)), ((), ())), preferred_element_type=F32)


def tn(a, b):
    return lax.dot_general(a, b, (((0,), (0,)), ((), ())), preferred_element_type=F32)


def split(v):
    high = v.astype(BF16)
    return high, (v - high.astype(F32)).astype(BF16)


def step_kernel(
    tok_ref, gain_ref, wq_ref, wk_ref, wv_ref, wg_ref, gin_ref, gf_ref, bias_ref, wo_ref,
    mem_ref, norm_ref, stab_ref, pk_ref, pv_ref, pin_ref, pf_ref, acc_ref,
    terms_ref, mem_out, norm_out, stab_out, keys_ref, values_ref,
    wbuf, wob, tok_own, tok_mid, tokbuf, tg, pbuf, rbuf, sbuf, srecv, memv, gin_v, gf_v, gbuf, ebuf,
    gain_v, norm_v, stab_v, pk_v, pv_v, pin_v, pf_v, acc_v, bias_v, coef, norm8,
    loc_sem, xs_sem, xr_sem, ys_sem, yr_sem, ts_sem, tr_sem, rs_sem, rr_sem, ss_sem, sr_sem,
    gs_sem, gr_sem, es_sem, er_sem,
):
    z, x = lax.axis_index("z"), lax.axis_index("x")
    y, c = lax.axis_index("y"), lax.axis_index("c")
    j = y * NC + c
    right, left = lax.rem(x + 1, NX), lax.rem(x + NX - 1, NX)
    opposite = lax.rem(x + 2, NX)
    zs = [lax.rem(z + d, NZ) for d in range(NZ)]
    js = [lax.rem(j + d, NJ) for d in range(NJ)]
    ys = [lax.rem(y + d, NY) for d in range(NY)]
    self_tok = j == z

    def at_x(other):
        return (z, other, y, c)

    def at_z(other):
        return (other, x, y, c)

    def at_y(other):
        return (z, x, other, c)

    def at_zj(other, tp):
        return (other, x, lax.div(tp, NC), lax.rem(tp, NC))

    def rdma(src, dst, ssem, rsem, dev):
        return pltpu.make_async_remote_copy(
            src_ref=src, dst_ref=dst, send_sem=ssem, recv_sem=rsem,
            device_id=dev, device_id_type=MESH,
        )

    def wblock(p, owner, start, size):
        if p < 8:
            first = pl.multiple_of(owner * 128 + start * 32, 32)
            return wbuf.at[p, pl.ds(first, size * 32), :]
        cols = pl.ds(pl.multiple_of(owner * 128, 128), 128)
        return wob.at[pl.ds(start * 128, size * 128), cols]

    feats = pl.ds(pl.multiple_of(z * 512, 512), 512)
    moves = (
        *(
            (w.at[:, pl.ds(h * DK, DK)], wblock(2 * i + h, x, 0, 4))
            for i, w in enumerate((wq_ref, wk_ref, wv_ref, wg_ref))
            for h in range(2)
        ),
        (wo_ref, wblock(8, x, 0, 4)), (tok_ref, tok_own), (gin_ref.at[:, feats], gin_v), (gf_ref.at[:, feats], gf_v), (mem_ref, mem_out),
        (gain_ref, gain_v), (norm_ref, norm_v), (stab_ref, stab_v), (pk_ref, pk_v), (pv_ref, pv_v),
        (pin_ref, pin_v), (pf_ref, pf_v), (acc_ref, acc_v), (bias_ref, bias_v),
    )
    local = [pltpu.make_async_copy(src, dst, loc_sem.at[i]) for i, (src, dst) in enumerate(moves)]
    for i in (0, 9, 1, 2, 3, 4, 5, 6, 7, 15, 18, 19, 20, 13, 14, 16, 17, 10, 11, 21, 8, 12):
        local[i].start()

    barrier = pltpu.get_barrier_semaphore()

    def greet(dev):
        pl.semaphore_signal(barrier, inc=1, device_id=dev, device_id_type=MESH)

    greet(at_x(right))
    greet(at_x(left))
    for d in range(1, NZ):
        greet(at_z(zs[d]))
        greet((zs[d], x, y, 1 - c))
    for d in range(1, NJ):
        greet(at_zj(z, js[d]))
    pl.semaphore_wait(barrier, 23)

    def direct(p):
        return [
            rdma(wblock(p, x, 0, 4), wblock(p, x, 0, 4), xs_sem.at[p, 0], xr_sem.at[p, 0], at_x(right)),
            rdma(wblock(p, x, 0, 4), wblock(p, x, 0, 4), xs_sem.at[p, 1], xr_sem.at[p, 1], at_x(left)),
        ]

    def onward(p):
        return [
            rdma(wblock(p, left, 0, 2), wblock(p, left, 0, 2), xs_sem.at[p, 2], xr_sem.at[p, 2], at_x(right)),
            rdma(wblock(p, right, 2, 2), wblock(p, right, 2, 2), xs_sem.at[p, 3], xr_sem.at[p, 3], at_x(left)),
        ]

    def arrive(p, which):
        owner, start, size = ((left, 0, 4), (right, 0, 4), (opposite, 0, 2), (opposite, 2, 2))[which]
        block = wblock(p, owner, start, size)
        rdma(block, block, xs_sem.at[p, which], xr_sem.at[p, which], at_x(left)).wait_recv()

    sent = []

    def go(copies):
        for copy in copies:
            copy.start()
            sent.append(copy)

    def forward(p):
        arrive(p, 0)
        arrive(p, 1)
        go(onward(p))
        if p < 5:
            local[p + 3].wait()
            go(direct(p + 3))

    local[0].wait()
    go(direct(0))
    local[9].wait()
    go([rdma(tok_own, tok_mid.at[y], ys_sem.at[d], yr_sem.at[y], at_y(ys[d])) for d in (2, 1, 3)])
    for p in (1, 2):
        local[p].wait()
        go(direct(p))

    for i in (15, 18, 19, 20):
        local[i].wait()
    taken = acc_v[...]
    stab = stab_v[...]
    logs, run = [], None
    for i in range(4):
        f = jnp.where(i < taken, log_sigmoid(pf_v[i]), 0.0)
        run = f if run is None else run + f
        logs.append(run)
    ends = [run - logs[i] + pin_v[i] for i in range(4)]
    stab_new = run + stab
    for i in range(4):
        stab_new = jnp.where(i < taken, jnp.maximum(stab_new, ends[i]), stab_new)
    stab_out[...] = stab_new
    for i in range(4):
        w = jnp.where(i < taken, jnp.exp(ends[i] - stab_new), 0.0) * (DK**-0.5)
        for h in range(2):
            coef[4 * h + i : 4 * h + i + 1, :] = w[h : h + 1]
    coef[8:10, :] = jnp.exp(run + stab - stab_new)
    coef[10:16, :] = jnp.zeros((6, 8), F32)
    coef_lane = lax.broadcasted_iota(jnp.int32, (16, 8), 1)
    for i in (12, 14, 16, 17):
        local[i].wait()

    def update(s, carry_in):
        col = jnp.sum(jnp.where(coef_lane == s, coef[...], 0.0), axis=1, keepdims=True)
        for h in range(2):
            cols = slice(h * DK, (h + 1) * DK)
            weighted = pk_v[s, :, cols].astype(F32) * col[4 * h : 4 * h + 4]
            carry = col[8 + h : 9 + h]
            high, low = split(weighted)
            vals = pv_v[s, :, cols]
            new = carry * mem_out[s, h] + (tn(high, vals) + tn(low, vals))
            mem_out[s, h] = new
            memv[s, h] = new.astype(BF16)
            row = carry * norm_v[s, h : h + 1] + jnp.sum(weighted, axis=0, keepdims=True)
            norm_out[s, h : h + 1] = row
            norm8[h, pl.ds(s, 1), :] = row
        return carry_in

    forward(0)

    relay_tok = []
    for d in (0, 1, 3, 2):
        far = ys[d] * NC + c
        block = tok_own if d == 0 else tok_mid.at[ys[d]]
        if d:
            rdma(tok_own, block, ys_sem.at[d], yr_sem.at[ys[d]], at_y(ys[d])).wait_recv()
        for core in range(NC):
            copy = rdma(
                block, tokbuf.at[z], ts_sem.at[2 * d + core], tr_sem.at[z],
                (far, x, y, lax.rem(c + core, NC)),
            )
            relay_tok.append((copy, far))

            @pl.when(jnp.logical_not((far == z) & (core == 0)))
            def _(copy=copy):
                copy.start()

        @pl.when(far == z)
        def _(block=block):
            tokbuf[z] = block[...]

    forward(1)
    lax.fori_loop(0, 2, update, 0)
    forward(2)
    lax.fori_loop(2, 4, update, 0)
    forward(3)
    lax.fori_loop(4, 6, update, 0)
    forward(4)
    lax.fori_loop(6, 8, update, 0)
    local[13].wait()
    gains = jnp.concatenate([gain_v[pl.ds(4 * z + r, 1), :] for r in range(4)], axis=1)

    def token_block(d):
        slot = zs[d]
        landed = rdma(tok_own, tokbuf.at[slot], ts_sem.at[d], tr_sem.at[slot], at_z(zs[1]))
        if d:
            landed.wait_recv()
        else:
            @pl.when(lax.rem(z, NC) != c)
            def _():
                landed.wait_recv()
        scaled = (tokbuf[slot].astype(F32) * gains).astype(BF16)
        tg[pl.ds(pl.multiple_of(slot * ROWS, ROWS), ROWS), :] = scaled

    for d in (0, 1, 7, 2, 6):
        token_block(d)
    forward(5)
    for d in (3, 5, 4):
        token_block(d)
    far_first = (4, 3, 5, 2, 6, 1, 7)
    def hop(p, block, slot, to):
        return rdma(block, rbuf.at[p, slot], rs_sem.at[p, slot], rr_sem.at[p, slot], at_z(zs[to]))

    def landed(p, slot):
        hop(p, pbuf.at[p, z], slot, 1).wait_recv()
        return rbuf[p, slot].astype(F32)

    def project(p):
        arrive(p, 2)
        arrive(p, 3)
        part = jnp.dot(tg[...], wbuf[p], preferred_element_type=F32)
        pbuf[p] = part.astype(BF16).reshape(NZ, ROWS, DK)
        if MODES[p] == 1:
            go([hop(p, pbuf.at[p, zs[d]], d, d) for d in far_first])
            return
        go([
            hop(p, pbuf.at[p, zs[4]], 4, 2 if p % 2 else 6),
            hop(p, pbuf.at[p, zs[3]], 3, 1),
            hop(p, pbuf.at[p, zs[5]], 5, 7),
        ])
        if MODES[p] == 2:
            go([hop(p, pbuf.at[p, zs[1]], 1, 1), hop(p, pbuf.at[p, zs[7]], 7, 7)])

    def pass_on(p, target, via, terms):
        total = pbuf[p, zs[target]].astype(F32)
        for slot in terms:
            total = total + landed(p, slot)
        pbuf[p, zs[target]] = total.astype(BF16)
        go([hop(p, pbuf.at[p, zs[target]], target, via)])

    def relay(p):
        far = MODES[p] == 2
        pass_on(p, 2, 2 if far else 1, (3, 4) if p % 2 else (3,))
        pass_on(p, 6, 6 if far else 7, (5,) if p % 2 else (5, 4))

    def relay_near(p):
        pass_on(p, 1, 1, (2,))
        pass_on(p, 7, 7, (6,))

    def collect(p):
        total = pbuf[p, z].astype(F32)
        for slot in ((1, 7, 2, 6, 3, 5, 4), (1, 7, 2, 6), (1, 7))[MODES[p] - 1]:
            total = total + landed(p, slot)
        return (total * scale_col).astype(BF16)

    small = []

    def send_small():
        row8 = lax.broadcasted_iota(jnp.int32, (8, 16), 0)
        lane16 = lax.broadcasted_iota(jnp.int32, (8, 16), 1)
        pick_in = jnp.where((row8 < 2) & (lane16 == 2 * j + row8), 1.0, 0.0).astype(BF16)
        pick_f = jnp.where((row8 >= 2) & (row8 < 4) & (lane16 == 2 * j + row8 - 2), 1.0, 0.0).astype(BF16)
        local[10].wait()
        local[11].wait()
        gates8 = (
            jnp.dot(pick_in, gin_v[...], preferred_element_type=F32)
            + jnp.dot(pick_f, gf_v[...], preferred_element_type=F32)
        ).astype(BF16)
        ones8 = jnp.full((8, 512), 1.0, BF16)
        row_all = lax.broadcasted_iota(jnp.int32, (8, NZ * ROWS), 0)
        sbuf[...] = jnp.zeros_like(sbuf)
        raw = tokbuf[...].astype(F32).reshape(NZ * ROWS, 512)
        high, low = split(raw * raw)
        squares = nt(ones8, high) + nt(ones8, low)
        rows = jnp.where(row_all == 4, squares, nt(gates8, tg[...]))
        for i in range(NZ):
            sbuf[i, :, 0:ROWS] = rows[:, i * ROWS : (i + 1) * ROWS]
        small.extend(
            rdma(sbuf.at[zs[d]], srecv.at[d], ss_sem.at[d], sr_sem.at[d], at_z(zs[d])) for d in far_first
        )
        go(small)

    for op in ORDER.split():
        if op == "S":
            send_small()
        elif op == "D":
            local[8].wait()
            go(direct(8))
        else:
            {"P": project, "B": relay, "C": relay_near, "F": forward}[op[0]](int(op[1]))

    for copy in small:
        copy.wait_recv()
    sums = sbuf[z]
    for d in range(1, NZ):
        sums = sums + srecv[d]
    scale_row = lax.rsqrt(sums[4:5, 0:ROWS] / D + EPS)
    ri = lax.broadcasted_iota(jnp.int32, (ROWS, ROWS), 0)
    ci = lax.broadcasted_iota(jnp.int32, (ROWS, ROWS), 1)
    eye = ri == ci
    same = lax.div(ri, 4) == lax.div(ci, 4)
    causal = same & (ci <= ri)
    anti = same & (ri <= ci)

    def to_col(row):
        return jnp.sum(jnp.where(eye, row, 0.0), axis=1, keepdims=True)

    scale_col = to_col(scale_row)
    seq_of_row = lax.div(lax.broadcasted_iota(jnp.int32, (ROWS, 8), 0), 4)
    seq_lane = lax.broadcasted_iota(jnp.int32, (ROWS, 8), 1)
    own_seq = seq_of_row == seq_lane
    row_seq = lax.div(lax.broadcasted_iota(jnp.int32, (ROWS, DK), 0), 4)

    queries, keys, values, carried_rows = [], [], [], []
    for h in range(2):
        q = collect(h)
        queries.append(q)
        read = jnp.zeros((ROWS, DK), F32)
        for s in range(8):
            part = jnp.dot(q, memv[s, h], preferred_element_type=F32)
            read = jnp.where(row_seq == s, part, read)
        carried_rows.append(read)
    for h in range(2):
        keys.append(collect(2 + h))
        keys_ref[:, h * DK : (h + 1) * DK] = keys[h]
    for h in range(2):
        values.append(collect(4 + h))
        values_ref[:, h * DK : (h + 1) * DK] = values[h]

    local[21].wait()
    bias_lane = lax.broadcasted_iota(jnp.int32, (1, 16), 1)
    hidden = []
    for h in range(2):
        q, k, v = queries[h], keys[h], values[h]
        bias = jnp.sum(jnp.where(bias_lane == 2 * j + h, bias_v[...], 0.0), axis=1, keepdims=True)
        in_row = sums[h : h + 1, 0:ROWS] * scale_row
        f_row = log_sigmoid(sums[2 + h : 3 + h, 0:ROWS] * scale_row + bias)
        f_col = to_col(f_row)
        b_col = jnp.sum(jnp.where(causal, f_row, 0.0), axis=1, keepdims=True)
        b_row = jnp.sum(jnp.where(anti, f_col, 0.0), axis=0, keepdims=True)
        within = jnp.where(causal, b_col - b_row + in_row, -jnp.inf)
        stab_col = jnp.sum(jnp.where(own_seq, stab_out[h : h + 1, :], 0.0), axis=1, keepdims=True)
        g_col = b_col + stab_col
        level = jnp.maximum(g_col, jnp.max(within, axis=1, keepdims=True))
        u = jnp.exp(g_col - level)
        w = nt(q, k) * (DK**-0.5) * jnp.where(causal, jnp.exp(within - level), 0.0)
        w_high, w_low = split(w)
        n_high, n_low = split(norm8[h])
        q_norm = jnp.sum(jnp.where(own_seq, nt(q, n_high) + nt(q, n_low), 0.0), axis=1, keepdims=True)
        num = u * carried_rows[h] + (
            jnp.dot(w_high, v, preferred_element_type=F32) + jnp.dot(w_low, v, preferred_element_type=F32)
        )
        den = u * q_norm + jnp.sum(w, axis=1, keepdims=True)
        hidden.append(num / jnp.maximum(jnp.abs(den), 1.0))

    arrive(8, 0)
    arrive(8, 1)
    go(onward(8))
    for h in range(2):
        gate = jax.nn.sigmoid(collect(6 + h).astype(F32))
        gbuf[h, z] = (gate * hidden[h]).astype(BF16)
        go([
            rdma(gbuf.at[h, z], gbuf.at[h, z], gs_sem.at[h, d], gr_sem.at[h, d], at_z(zs[d]))
            for d in far_first
        ])
    arrive(8, 2)
    arrive(8, 3)

    for d in (0, 1, 7, 2, 6, 3, 5, 4):
        slot = zs[d]
        out = jnp.zeros((ROWS, 512), F32)
        for h in range(2):
            if d:
                came = NZ - d
                rdma(
                    gbuf.at[h, slot], gbuf.at[h, slot], gs_sem.at[h, came], gr_sem.at[h, came], at_z(slot)
                ).wait_recv()
            out = out + jnp.dot(gbuf[h, slot], wob[h * DK : (h + 1) * DK, :], preferred_element_type=F32)
        ebuf[slot] = out.astype(BF16)
        out = rdma(ebuf.at[slot], terms_ref.at[j], es_sem.at[d], er_sem.at[j], at_zj(slot, z))
        if d:
            go([out])
        else:
            own_out = out

            @pl.when(jnp.logical_not(self_tok))
            def _():
                own_out.start()

            @pl.when(self_tok)
            def _():
                terms_ref[j] = ebuf[slot]

    for d in range(NJ):
        slot = js[d]
        came = rdma(ebuf.at[0], terms_ref.at[slot], es_sem.at[d], er_sem.at[slot], at_zj(z, slot))
        if d:
            came.wait_recv()
        else:
            @pl.when(jnp.logical_not(self_tok))
            def _(came=came):
                came.wait_recv()

    for copy in sent:
        copy.wait_send()
    for i, (copy, far) in enumerate(relay_tok):
        @pl.when(jnp.logical_not((far == z) & (i % 2 == 0)))
        def _(copy=copy):
            copy.wait_send()

    @pl.when(jnp.logical_not(self_tok))
    def _():
        own_out.wait_send()


def finish_kernel(terms, mem, norm, stab, keys, values, mixed, mem_o, norm_o, stab_o, keys_o, values_o, total_v, sem):
    pairs = ((mem, mem_o), (norm, norm_o), (stab, stab_o), (keys, keys_o), (values, values_o), (total_v, mixed))
    copies = [pltpu.make_async_copy(src, dst, sem.at[i]) for i, (src, dst) in enumerate(pairs)]
    for copy in copies[1:5]:
        copy.start()
    total = terms[0].astype(F32)
    for i in range(1, NJ):
        total = total + terms[i].astype(F32)
    total_v[...] = total.astype(BF16)
    copies[0].start()
    copies[5].start()
    for copy in copies:
        copy.wait()


def step(*args):
    args = [pltpu.with_memory_space_constraint(a, pltpu.HBM) for a in args]
    hbm = pl.BlockSpec(memory_space=pltpu.HBM)
    vmem = pl.BlockSpec(memory_space=pltpu.VMEM)
    dma = pltpu.SemaphoreType.DMA
    block = lambda *lead: pltpu.VMEM((*lead, ROWS, 512), BF16)
    shape = jax.ShapeDtypeStruct
    outs = [
        shape((NJ, ROWS, 512), BF16), shape((8, 2, DK, DK), F32), shape((8, 2, DK), F32),
        shape((2, 8), F32), shape((ROWS, 512), BF16), shape((ROWS, 512), BF16),
    ]
    parts = pl.pallas_call(
        step_kernel,
        in_specs=[hbm] * 18,
        out_specs=[vmem] * 6,
        out_shape=outs,
        scratch_shapes=[
            pltpu.VMEM((8, 512, DK), BF16),
            pltpu.VMEM((512, 512), BF16),
            block(),
            block(NY),
            block(NZ),
            pltpu.VMEM((256, 512), BF16),
            pltpu.VMEM((8, NZ, ROWS, DK), BF16),
            pltpu.VMEM((8, NZ, ROWS, DK), BF16),
            pltpu.VMEM((NZ, 8, 128), F32),
            pltpu.VMEM((NZ, 8, 128), F32),
            pltpu.VMEM((8, 2, DK, DK), BF16),
            pltpu.VMEM((16, 512), BF16),
            pltpu.VMEM((16, 512), BF16),
            pltpu.VMEM((2, NZ, ROWS, DK), BF16),
            block(NZ),
            pltpu.VMEM((32, 128), F32),
            pltpu.VMEM((8, 2, DK), F32),
            pltpu.VMEM((2, 8), F32),
            pltpu.VMEM((8, 4, 512), BF16),
            pltpu.VMEM((8, 4, 512), BF16),
            pltpu.VMEM((4, 2, 8), F32),
            pltpu.VMEM((4, 2, 8), F32),
            pltpu.VMEM((1, 8), jnp.int32),
            pltpu.VMEM((1, 16), F32),
            pltpu.VMEM((16, 8), F32),
            pltpu.VMEM((2, 8, DK), F32),
            dma((22,)), dma((9, 4)), dma((9, 4)), dma((4,)), dma((4,)), dma((8,)), dma((8,)),
            dma((8, 8)), dma((8, 8)), dma((8,)), dma((8,)), dma((2, 8)), dma((2, 8)), dma((8,)), dma((8,)),
        ],
        compiler_params=pltpu.CompilerParams(
            collective_id=0, has_side_effects=True, vmem_limit_bytes=24 * 1024 * 1024
        ),
        name="step",
    )(*args)
    return pl.pallas_call(
        finish_kernel,
        in_specs=[vmem] + [pl.BlockSpec(memory_space=pl.ANY)] * 5,
        out_specs=[hbm] * 6,
        out_shape=[shape((ROWS, 512), BF16)] + outs[1:],
        scratch_shapes=[pltpu.VMEM((ROWS, 512), BF16), dma((6,))],
        name="finish",
        compiler_params=pltpu.CompilerParams(vmem_limit_bytes=4 * 1024 * 1024),
    )(*[pltpu.with_memory_space_constraint(part, pltpu.VMEM) for part in parts])


def body(
    tokens, norm_gain, query_weight, key_weight, value_weight, outgate_weight, ingate_weight,
    forget_weight, forget_bias, output_weight, state_memory, state_normaliser, state_stabiliser,
    past_keys, past_values, past_ingate, past_forget, accepted,
):
    mixed, memory, normaliser, stab_t, keys, values = step(
        tokens, norm_gain.reshape(32, 128), query_weight, key_weight, value_weight, outgate_weight,
        ingate_weight.T, forget_weight.T, forget_bias.reshape(1, 16), output_weight,
        state_memory, state_normaliser, state_stabiliser.T, past_keys, past_values,
        past_ingate.transpose(1, 2, 0), past_forget.transpose(1, 2, 0), accepted.reshape(1, 8),
    )
    return (mixed, memory, normaliser, stab_t.T, keys, values)


def solution(mesh):
    torus = Mesh(mesh.devices.reshape(NZ, NX, NY, NC), ("z", "x", "y", "c"))
    kv, tp = ("z", "x"), ("y", "c")
    in_specs = (
        P(kv, tp), P(), P(kv, tp), P(kv, tp), P(kv, tp), P(kv, tp), P(), P(), P(), P(tp, kv),
        P(kv, tp, None, None), P(kv, tp, None), P(kv, tp), P(kv, None, tp), P(kv, None, tp),
        P(kv, None, tp), P(kv, None, tp), P(kv),
    )
    out_specs = (
        P(kv, tp), P(kv, tp, None, None), P(kv, tp, None), P(kv, tp), P(kv, tp), P(kv, tp),
    )
    return jax.shard_map(body, mesh=torus, in_specs=in_specs, out_specs=out_specs, check_vma=False)
```

```python
import jax
import jax.numpy as jnp
from jax import lax
from jax.experimental import pallas as pl
from jax.experimental.pallas import tpu as pltpu
from jax.sharding import Mesh
from jax.sharding import PartitionSpec as P

D = 4096
DK = 256
NZ, NX, NY, NC = 8, 4, 4, 2
NJ = NY * NC
ROWS = 32
EPS = 1e-06
RELAYED = 3
PIECES = ((0, True), (1, True), (2, True), (0, False), (1, False), (2, False), (3, True), (3, False))
MESH = pl.DeviceIdType.MESH
F32 = jnp.float32
BF16 = jnp.bfloat16


def log_sigmoid(v):
    return jnp.minimum(v, 0.0) - jnp.log1p(jnp.exp(-jnp.abs(v)))


def nt(a, b):
    return lax.dot_general(a, b, (((1,), (1,)), ((), ())), preferred_element_type=F32)


def tn(a, b):
    return lax.dot_general(a, b, (((0,), (0,)), ((), ())), preferred_element_type=F32)


def split(v):
    high = v.astype(BF16)
    return high, (v - high.astype(F32)).astype(BF16)


def step_kernel(
    tok_ref, gain_ref, wq_ref, wk_ref, wv_ref, wg_ref, gin_ref, gf_ref, bias_ref, wo_ref,
    mem_ref, norm_ref, stab_ref, pk_ref, pv_ref, pin_ref, pf_ref, acc_ref,
    terms_ref, mem_out, norm_out, stab_out, keys_ref, values_ref,
    wbuf, swap, wob, tok_own, tok_mid, tokbuf, tg, pbuf, rbuf, sbuf, srecv, memv, gin_v, gf_v, gbuf, ebuf,
    gain_v, norm_v, stab_v, pk_v, pv_v, pin_v, pf_v, acc_v, bias_v, coef, norm8,
    loc_sem, xs_sem, xr_sem, ws_sem, wr_sem, fs_sem, fr_sem, ys_sem, yr_sem, ts_sem, tr_sem, rs_sem, rr_sem, ss_sem, sr_sem,
    gs_sem, gr_sem, es_sem, er_sem,
):
    z, x = lax.axis_index("z"), lax.axis_index("x")
    y, c = lax.axis_index("y"), lax.axis_index("c")
    j = y * NC + c
    right, left = lax.rem(x + 1, NX), lax.rem(x + NX - 1, NX)
    opposite = lax.rem(x + 2, NX)
    zs = [lax.rem(z + d, NZ) for d in range(NZ)]
    js = [lax.rem(j + d, NJ) for d in range(NJ)]
    ys = [lax.rem(y + d, NY) for d in range(NY)]
    self_tok = j == z
    even = lax.rem(z, 2)
    odd = 1 - even
    partner = z + 1 - 2 * even
    base = z - even

    def at_x(other):
        return (z, other, y, c)

    def at_z(other):
        return (other, x, y, c)

    def at_y(other):
        return (z, x, other, c)

    def at_zj(other, tp):
        return (other, x, lax.div(tp, NC), lax.rem(tp, NC))

    def rdma(src, dst, ssem, rsem, dev):
        return pltpu.make_async_remote_copy(
            src_ref=src, dst_ref=dst, send_sem=ssem, recv_sem=rsem,
            device_id=dev, device_id_type=MESH,
        )

    own_cols = pl.ds(pl.multiple_of(even * DK, DK), DK)
    other_cols = pl.ds(pl.multiple_of(odd * DK, DK), DK)

    def wblock(piece, owner, start, size):
        if piece < 8:
            proj, own = PIECES[piece]
            first = pl.multiple_of(owner * 128 + start * 32, 32)
            return wbuf.at[proj, even if own else odd, pl.ds(first, size * 32), :]
        cols = pl.ds(pl.multiple_of(owner * 128, 128), 128)
        return wob.at[pl.ds(start * 128, size * 128), cols]

    feats = pl.ds(pl.multiple_of(z * 512, 512), 512)
    moves = (
        (wq_ref.at[:, own_cols], wblock(0, x, 0, 4)), (wk_ref.at[:, own_cols], wblock(1, x, 0, 4)),
        (wv_ref.at[:, own_cols], wblock(2, x, 0, 4)), (wg_ref.at[:, own_cols], wblock(6, x, 0, 4)),
        (wq_ref.at[:, other_cols], swap.at[0]), (wk_ref.at[:, other_cols], swap.at[1]),
        (wv_ref.at[:, other_cols], swap.at[2]), (wg_ref.at[:, other_cols], swap.at[3]),
        (wo_ref, wblock(8, x, 0, 4)), (tok_ref, tok_own), (gin_ref.at[:, feats], gin_v), (gf_ref.at[:, feats], gf_v), (mem_ref, mem_out),
        (gain_ref, gain_v), (norm_ref, norm_v), (stab_ref, stab_v), (pk_ref, pk_v), (pv_ref, pv_v),
        (pin_ref, pin_v), (pf_ref, pf_v), (acc_ref, acc_v), (bias_ref, bias_v),
    )
    local = [pltpu.make_async_copy(src, dst, loc_sem.at[i]) for i, (src, dst) in enumerate(moves)]
    for i in (0, 9, 4, 1, 2, 5, 6, 7, 3, 15, 18, 19, 20, 13, 14, 16, 17, 10, 11, 21, 8, 12):
        local[i].start()

    barrier = pltpu.get_barrier_semaphore()

    def greet(dev):
        pl.semaphore_signal(barrier, inc=1, device_id=dev, device_id_type=MESH)

    greet(at_x(right))
    greet(at_x(left))
    for d in range(1, NZ):
        greet(at_z(zs[d]))
        greet((zs[d], x, y, 1 - c))
    for d in range(1, NJ):
        greet(at_zj(z, js[d]))
    pl.semaphore_wait(barrier, 23)

    def direct(p):
        return [
            rdma(wblock(p, x, 0, 4), wblock(p, x, 0, 4), xs_sem.at[p, 0], xr_sem.at[p, 0], at_x(right)),
            rdma(wblock(p, x, 0, 4), wblock(p, x, 0, 4), xs_sem.at[p, 1], xr_sem.at[p, 1], at_x(left)),
        ]

    def onward(p):
        return [
            rdma(wblock(p, left, 0, 2), wblock(p, left, 0, 2), xs_sem.at[p, 2], xr_sem.at[p, 2], at_x(right)),
            rdma(wblock(p, right, 2, 2), wblock(p, right, 2, 2), xs_sem.at[p, 3], xr_sem.at[p, 3], at_x(left)),
        ]

    def arrive(p, which):
        owner, start, size = ((left, 0, 4), (right, 0, 4), (opposite, 0, 2), (opposite, 2, 2))[which]
        block = wblock(p, owner, start, size)
        rdma(block, block, xs_sem.at[p, which], xr_sem.at[p, which], at_x(left)).wait_recv()

    sent = []

    def go(copies):
        for copy in copies:
            copy.start()
            sent.append(copy)

    def give(proj):
        mine = wbuf.at[proj, even, pl.ds(pl.multiple_of(x * 128, 128), 128), :]
        return rdma(swap.at[proj], mine, ws_sem.at[proj], wr_sem.at[proj], at_z(partner))

    def send(piece):
        if piece < 8:
            proj, own = PIECES[piece]
            if own:
                local[proj].wait()
            else:
                block = wblock(piece, x, 0, 4)
                rdma(swap.at[proj], block, ws_sem.at[proj], wr_sem.at[proj], at_z(partner)).wait_recv()
        else:
            local[8].wait()
        go(direct(piece))

    def forward(p):
        arrive(p, 0)
        arrive(p, 1)
        go(onward(p))
        if p < 5:
            send(p + 3)

    send(0)
    local[9].wait()
    go([rdma(tok_own, tok_mid.at[y], ys_sem.at[d], yr_sem.at[y], at_y(ys[d])) for d in (2, 1, 3)])
    relay_tok = []

    def spread(d):
        block = tok_own if d == 0 else tok_mid.at[ys[d]]
        if d:
            rdma(tok_own, block, ys_sem.at[d], yr_sem.at[ys[d]], at_y(ys[d])).wait_recv()
        same, cross = 2 * ys[d] + even, 2 * ys[d] + odd
        first = rdma(block, tokbuf.at[c, z], ts_sem.at[2 * d], tr_sem.at[z], at_z(same))
        go([rdma(block, tokbuf.at[c, z], ts_sem.at[2 * d + 1], tr_sem.at[z], at_z(cross))])
        relay_tok.append((first, same))

        @pl.when(same != z)
        def _():
            first.start()

        @pl.when(same == z)
        def _():
            tokbuf[c, z] = block[...]

    spread(0)
    for proj in range(4):
        local[4 + proj].wait()
        go([give(proj)])
        if proj < 2:
            send(proj + 1)

    for i in (15, 18, 19, 20):
        local[i].wait()
    taken = acc_v[...]
    stab = stab_v[...]
    logs, run = [], None
    for i in range(4):
        f = jnp.where(i < taken, log_sigmoid(pf_v[i]), 0.0)
        run = f if run is None else run + f
        logs.append(run)
    ends = [run - logs[i] + pin_v[i] for i in range(4)]
    stab_new = run + stab
    for i in range(4):
        stab_new = jnp.where(i < taken, jnp.maximum(stab_new, ends[i]), stab_new)
    stab_out[...] = stab_new
    for i in range(4):
        w = jnp.where(i < taken, jnp.exp(ends[i] - stab_new), 0.0) * (DK**-0.5)
        for h in range(2):
            coef[4 * h + i : 4 * h + i + 1, :] = w[h : h + 1]
    coef[8:10, :] = jnp.exp(run + stab - stab_new)
    coef[10:16, :] = jnp.zeros((6, 8), F32)
    coef_lane = lax.broadcasted_iota(jnp.int32, (16, 8), 1)
    for i in (12, 14, 16, 17):
        local[i].wait()

    def update(s, carry_in):
        col = jnp.sum(jnp.where(coef_lane == s, coef[...], 0.0), axis=1, keepdims=True)
        for h in range(2):
            cols = slice(h * DK, (h + 1) * DK)
            weighted = pk_v[s, :, cols].astype(F32) * col[4 * h : 4 * h + 4]
            carry = col[8 + h : 9 + h]
            high, low = split(weighted)
            vals = pv_v[s, :, cols]
            new = carry * mem_out[s, h] + (tn(high, vals) + tn(low, vals))
            mem_out[s, h] = new
            memv[s, h] = new.astype(BF16)
            row = carry * norm_v[s, h : h + 1] + jnp.sum(weighted, axis=0, keepdims=True)
            norm_out[s, h : h + 1] = row
            norm8[h, pl.ds(s, 1), :] = row
        return carry_in

    forward(0)

    for d in (1, 3, 2):
        spread(d)

    forward(1)
    lax.fori_loop(0, 2, update, 0)
    forward(2)
    lax.fori_loop(2, 4, update, 0)
    forward(3)
    lax.fori_loop(4, 6, update, 0)
    forward(4)
    lax.fori_loop(6, 8, update, 0)
    local[13].wait()

    def gains_of(plane):
        rows = [gain_v[pl.ds(4 * (base + plane) + r, 1), :] for r in range(4)]
        return jnp.concatenate(rows, axis=1)

    def crossing(core, slot):
        block = tokbuf.at[core, slot]
        return rdma(block, block, fs_sem.at[slot], fr_sem.at[slot], (z, x, y, 1 - c))

    def scale_block(core, slot, gains):
        scaled = (tokbuf[core, slot].astype(F32) * gains).astype(BF16)
        tg[core, pl.ds(pl.multiple_of(slot * ROWS, ROWS), ROWS), :] = scaled

    near_first = (0, 1, 7, 2, 6, 3, 5, 4)
    own_gains = gains_of(c)
    for d in near_first:
        slot = zs[d]
        if d:
            rdma(tok_own, tokbuf.at[c, slot], ts_sem.at[0], tr_sem.at[slot], at_z(slot)).wait_recv()
        go([crossing(c, slot)])
        scale_block(c, slot, own_gains)
    forward(5)
    other_gains = gains_of(1 - c)
    for d in near_first:
        slot = zs[d]
        crossing(1 - c, slot).wait_recv()
        scale_block(1 - c, slot, other_gains)
    far_first = (4, 3, 5, 2, 6, 1, 7)
    def hop(p, block, slot, to):
        return rdma(block, rbuf.at[p, slot], rs_sem.at[p, slot], rr_sem.at[p, slot], at_z(zs[to]))

    def landed(p, slot):
        hop(p, pbuf.at[p, z], slot, 1).wait_recv()
        return rbuf[p, slot].astype(F32)

    def project(p):
        for piece in range(8):
            if PIECES[piece][0] == p:
                arrive(piece, 2)
                arrive(piece, 3)
        part = jnp.dot(tg[0], wbuf[p, 0], preferred_element_type=F32)
        part = part + jnp.dot(tg[1], wbuf[p, 1], preferred_element_type=F32)
        pbuf[p] = part.astype(BF16).reshape(NZ, ROWS, DK)
        if p >= RELAYED:
            go([hop(p, pbuf.at[p, zs[d]], d, d) for d in far_first])
            return
        ahead, back = (2, 6) if p % 2 == 0 else (6, 2)
        go([
            hop(p, pbuf.at[p, zs[4]], 4, ahead),
            hop(p, pbuf.at[p, zs[3]], 3, 2),
            hop(p, pbuf.at[p, zs[5]], 5, 6),
            hop(p, pbuf.at[p, zs[back]], back, back),
        ])

    def pass_on(p, target, slot):
        total = pbuf[p, zs[target]].astype(F32) + landed(p, slot)
        pbuf[p, zs[target]] = total.astype(BF16)
        go([hop(p, pbuf.at[p, zs[target]], target, target)])

    def relay(p):
        pass_on(p, 1, 3)
        pass_on(p, 7, 5)
        pass_on(p, 2 if p % 2 == 0 else 6, 4)

    def collect(p):
        mine = pbuf[p, z].astype(F32)
        for slot in (2, 6) if p < RELAYED else (2, 6, 4):
            mine = mine + landed(p, slot)
        other = landed(p, 1)
        for slot in (7,) if p < RELAYED else (7, 3, 5):
            other = other + landed(p, slot)
        mine = (mine * scale_col).astype(BF16)
        other = (other * scale_col).astype(BF16)
        return jnp.where(even == 0, mine, other), jnp.where(even == 0, other, mine)

    small = []

    def send_small():
        row8 = lax.broadcasted_iota(jnp.int32, (8, 16), 0)
        lane16 = lax.broadcasted_iota(jnp.int32, (8, 16), 1)
        pick_in = jnp.where((row8 < 2) & (lane16 == 2 * j + row8), 1.0, 0.0).astype(BF16)
        pick_f = jnp.where((row8 >= 2) & (row8 < 4) & (lane16 == 2 * j + row8 - 2), 1.0, 0.0).astype(BF16)
        local[10].wait()
        local[11].wait()
        gates8 = (
            jnp.dot(pick_in, gin_v[...], preferred_element_type=F32)
            + jnp.dot(pick_f, gf_v[...], preferred_element_type=F32)
        ).astype(BF16)
        ones8 = jnp.full((8, 512), 1.0, BF16)
        row_all = lax.broadcasted_iota(jnp.int32, (8, NZ * ROWS), 0)
        sbuf[...] = jnp.zeros_like(sbuf)
        raw = tokbuf[even].astype(F32).reshape(NZ * ROWS, 512)
        high, low = split(raw * raw)
        squares = nt(ones8, high) + nt(ones8, low)
        rows = jnp.where(row_all == 4, squares, nt(gates8, tg[even]))
        for i in range(NZ):
            sbuf[i, :, 0:ROWS] = rows[:, i * ROWS : (i + 1) * ROWS]
        small.extend(
            rdma(sbuf.at[zs[d]], srecv.at[d], ss_sem.at[d], sr_sem.at[d], at_z(zs[d])) for d in far_first
        )
        go(small)

    project(0)
    forward(6)
    project(1)
    forward(7)
    send(8)
    project(2)
    send_small()
    relay(0)
    relay(1)
    project(3)
    relay(2)

    for copy in small:
        copy.wait_recv()
    sums = sbuf[z]
    for d in range(1, NZ):
        sums = sums + srecv[d]
    scale_row = lax.rsqrt(sums[4:5, 0:ROWS] / D + EPS)
    ri = lax.broadcasted_iota(jnp.int32, (ROWS, ROWS), 0)
    ci = lax.broadcasted_iota(jnp.int32, (ROWS, ROWS), 1)
    eye = ri == ci
    same = lax.div(ri, 4) == lax.div(ci, 4)
    causal = same & (ci <= ri)
    anti = same & (ri <= ci)

    def to_col(row):
        return jnp.sum(jnp.where(eye, row, 0.0), axis=1, keepdims=True)

    scale_col = to_col(scale_row)
    seq_of_row = lax.div(lax.broadcasted_iota(jnp.int32, (ROWS, 8), 0), 4)
    seq_lane = lax.broadcasted_iota(jnp.int32, (ROWS, 8), 1)
    own_seq = seq_of_row == seq_lane
    row_seq = lax.div(lax.broadcasted_iota(jnp.int32, (ROWS, DK), 0), 4)

    queries = collect(0)
    carried_rows = []
    for h in range(2):
        read = jnp.zeros((ROWS, DK), F32)
        for s in range(8):
            part = jnp.dot(queries[h], memv[s, h], preferred_element_type=F32)
            read = jnp.where(row_seq == s, part, read)
        carried_rows.append(read)
    keys = collect(1)
    values = collect(2)
    for h in range(2):
        keys_ref[:, h * DK : (h + 1) * DK] = keys[h]
        values_ref[:, h * DK : (h + 1) * DK] = values[h]

    local[21].wait()
    bias_lane = lax.broadcasted_iota(jnp.int32, (1, 16), 1)
    hidden = []
    for h in range(2):
        q, k, v = queries[h], keys[h], values[h]
        bias = jnp.sum(jnp.where(bias_lane == 2 * j + h, bias_v[...], 0.0), axis=1, keepdims=True)
        in_row = sums[h : h + 1, 0:ROWS] * scale_row
        f_row = log_sigmoid(sums[2 + h : 3 + h, 0:ROWS] * scale_row + bias)
        f_col = to_col(f_row)
        b_col = jnp.sum(jnp.where(causal, f_row, 0.0), axis=1, keepdims=True)
        b_row = jnp.sum(jnp.where(anti, f_col, 0.0), axis=0, keepdims=True)
        within = jnp.where(causal, b_col - b_row + in_row, -jnp.inf)
        stab_col = jnp.sum(jnp.where(own_seq, stab_out[h : h + 1, :], 0.0), axis=1, keepdims=True)
        g_col = b_col + stab_col
        level = jnp.maximum(g_col, jnp.max(within, axis=1, keepdims=True))
        u = jnp.exp(g_col - level)
        w = nt(q, k) * (DK**-0.5) * jnp.where(causal, jnp.exp(within - level), 0.0)
        w_high, w_low = split(w)
        n_high, n_low = split(norm8[h])
        q_norm = jnp.sum(jnp.where(own_seq, nt(q, n_high) + nt(q, n_low), 0.0), axis=1, keepdims=True)
        num = u * carried_rows[h] + (
            jnp.dot(w_high, v, preferred_element_type=F32) + jnp.dot(w_low, v, preferred_element_type=F32)
        )
        den = u * q_norm + jnp.sum(w, axis=1, keepdims=True)
        hidden.append(num / jnp.maximum(jnp.abs(den), 1.0))

    arrive(8, 0)
    arrive(8, 1)
    go(onward(8))
    pre = collect(3)
    for h in range(2):
        gbuf[h, z] = (jax.nn.sigmoid(pre[h].astype(F32)) * hidden[h]).astype(BF16)
    for h in range(2):
        go([
            rdma(gbuf.at[h, z], gbuf.at[h, z], gs_sem.at[h, d], gr_sem.at[h, d], at_z(zs[d]))
            for d in far_first
        ])
    arrive(8, 2)
    arrive(8, 3)

    for d in (0, 1, 7, 2, 6, 3, 5, 4):
        slot = zs[d]
        out = jnp.zeros((ROWS, 512), F32)
        for h in range(2):
            if d:
                came = NZ - d
                rdma(
                    gbuf.at[h, slot], gbuf.at[h, slot], gs_sem.at[h, came], gr_sem.at[h, came], at_z(slot)
                ).wait_recv()
            out = out + jnp.dot(gbuf[h, slot], wob[h * DK : (h + 1) * DK, :], preferred_element_type=F32)
        ebuf[slot] = out.astype(BF16)
        out = rdma(ebuf.at[slot], terms_ref.at[j], es_sem.at[d], er_sem.at[j], at_zj(slot, z))
        if d:
            go([out])
        else:
            own_out = out

            @pl.when(jnp.logical_not(self_tok))
            def _():
                own_out.start()

            @pl.when(self_tok)
            def _():
                terms_ref[j] = ebuf[slot]

    for d in range(NJ):
        slot = js[d]
        came = rdma(ebuf.at[0], terms_ref.at[slot], es_sem.at[d], er_sem.at[slot], at_zj(z, slot))
        if d:
            came.wait_recv()
        else:
            @pl.when(jnp.logical_not(self_tok))
            def _(came=came):
                came.wait_recv()

    for copy in sent:
        copy.wait_send()
    for copy, same in relay_tok:
        @pl.when(same != z)
        def _(copy=copy):
            copy.wait_send()

    @pl.when(jnp.logical_not(self_tok))
    def _():
        own_out.wait_send()


def finish_kernel(terms, mem, norm, stab, keys, values, mixed, mem_o, norm_o, stab_o, keys_o, values_o, total_v, sem):
    pairs = ((mem, mem_o), (norm, norm_o), (stab, stab_o), (keys, keys_o), (values, values_o), (total_v, mixed))
    copies = [pltpu.make_async_copy(src, dst, sem.at[i]) for i, (src, dst) in enumerate(pairs)]
    for copy in copies[1:5]:
        copy.start()
    total = terms[0].astype(F32)
    for i in range(1, NJ):
        total = total + terms[i].astype(F32)
    total_v[...] = total.astype(BF16)
    copies[0].start()
    copies[5].start()
    for copy in copies:
        copy.wait()


def step(*args):
    args = [pltpu.with_memory_space_constraint(a, pltpu.HBM) for a in args]
    hbm = pl.BlockSpec(memory_space=pltpu.HBM)
    vmem = pl.BlockSpec(memory_space=pltpu.VMEM)
    dma = pltpu.SemaphoreType.DMA
    block = lambda *lead: pltpu.VMEM((*lead, ROWS, 512), BF16)
    shape = jax.ShapeDtypeStruct
    outs = [
        shape((NJ, ROWS, 512), BF16), shape((8, 2, DK, DK), F32), shape((8, 2, DK), F32),
        shape((2, 8), F32), shape((ROWS, 512), BF16), shape((ROWS, 512), BF16),
    ]
    parts = pl.pallas_call(
        step_kernel,
        in_specs=[hbm] * 18,
        out_specs=[vmem] * 6,
        out_shape=outs,
        scratch_shapes=[
            pltpu.VMEM((4, 2, 512, DK), BF16),
            pltpu.VMEM((4, 128, DK), BF16),
            pltpu.VMEM((512, 512), BF16),
            block(),
            block(NY),
            block(2, NZ),
            pltpu.VMEM((2, 256, 512), BF16),
            pltpu.VMEM((4, NZ, ROWS, DK), BF16),
            pltpu.VMEM((4, NZ, ROWS, DK), BF16),
            pltpu.VMEM((NZ, 8, 128), F32),
            pltpu.VMEM((NZ, 8, 128), F32),
            pltpu.VMEM((8, 2, DK, DK), BF16),
            pltpu.VMEM((16, 512), BF16),
            pltpu.VMEM((16, 512), BF16),
            pltpu.VMEM((2, NZ, ROWS, DK), BF16),
            block(NZ),
            pltpu.VMEM((32, 128), F32),
            pltpu.VMEM((8, 2, DK), F32),
            pltpu.VMEM((2, 8), F32),
            pltpu.VMEM((8, 4, 512), BF16),
            pltpu.VMEM((8, 4, 512), BF16),
            pltpu.VMEM((4, 2, 8), F32),
            pltpu.VMEM((4, 2, 8), F32),
            pltpu.VMEM((1, 8), jnp.int32),
            pltpu.VMEM((1, 16), F32),
            pltpu.VMEM((16, 8), F32),
            pltpu.VMEM((2, 8, DK), F32),
            dma((22,)), dma((9, 4)), dma((9, 4)), dma((4,)), dma((4,)), dma((8,)), dma((8,)),
            dma((4,)), dma((4,)), dma((8,)), dma((8,)),
            dma((4, 8)), dma((4, 8)), dma((8,)), dma((8,)), dma((2, 8)), dma((2, 8)), dma((8,)), dma((8,)),
        ],
        compiler_params=pltpu.CompilerParams(
            collective_id=0, has_side_effects=True, vmem_limit_bytes=24 * 1024 * 1024
        ),
        name="step",
    )(*args)
    return pl.pallas_call(
        finish_kernel,
        in_specs=[vmem] + [pl.BlockSpec(memory_space=pl.ANY)] * 5,
        out_specs=[hbm] * 6,
        out_shape=[shape((ROWS, 512), BF16)] + outs[1:],
        scratch_shapes=[pltpu.VMEM((ROWS, 512), BF16), dma((6,))],
        name="finish",
        compiler_params=pltpu.CompilerParams(vmem_limit_bytes=4 * 1024 * 1024),
    )(*[pltpu.with_memory_space_constraint(part, pltpu.VMEM) for part in parts])


def body(
    tokens, norm_gain, query_weight, key_weight, value_weight, outgate_weight, ingate_weight,
    forget_weight, forget_bias, output_weight, state_memory, state_normaliser, state_stabiliser,
    past_keys, past_values, past_ingate, past_forget, accepted,
):
    mixed, memory, normaliser, stab_t, keys, values = step(
        tokens, norm_gain.reshape(32, 128), query_weight, key_weight, value_weight, outgate_weight,
        ingate_weight.T, forget_weight.T, forget_bias.reshape(1, 16), output_weight,
        state_memory, state_normaliser, state_stabiliser.T, past_keys, past_values,
        past_ingate.transpose(1, 2, 0), past_forget.transpose(1, 2, 0), accepted.reshape(1, 8),
    )
    return (mixed, memory, normaliser, stab_t.T, keys, values)


def solution(mesh):
    torus = Mesh(mesh.devices.reshape(NZ, NX, NY, NC), ("z", "x", "y", "c"))
    kv, tp = ("z", "x"), ("y", "c")
    in_specs = (
        P(kv, tp), P(), P(kv, tp), P(kv, tp), P(kv, tp), P(kv, tp), P(), P(), P(), P(tp, kv),
        P(kv, tp, None, None), P(kv, tp, None), P(kv, tp), P(kv, None, tp), P(kv, None, tp),
        P(kv, None, tp), P(kv, None, tp), P(kv),
    )
    out_specs = (
        P(kv, tp), P(kv, tp, None, None), P(kv, tp, None), P(kv, tp), P(kv, tp), P(kv, tp),
    )
    return jax.shard_map(body, mesh=torus, in_specs=in_specs, out_specs=out_specs, check_vma=False)
```

```python
import jax
import jax.numpy as jnp
from jax import lax
from jax.experimental import pallas as pl
from jax.experimental.pallas import tpu as pltpu
from jax.sharding import Mesh
from jax.sharding import PartitionSpec as P

D = 4096
DK = 256
NZ, NX, NY, NC = 8, 4, 4, 2
NJ = NY * NC
ROWS = 32
EPS = 1e-06
RELAYED = 2
PIECES = ((0, True), (1, True), (2, True), (0, False), (1, False), (2, False), (3, True), (3, False))
MESH = pl.DeviceIdType.MESH
F32 = jnp.float32
BF16 = jnp.bfloat16


def log_sigmoid(v):
    return jnp.minimum(v, 0.0) - jnp.log1p(jnp.exp(-jnp.abs(v)))


def nt(a, b):
    return lax.dot_general(a, b, (((1,), (1,)), ((), ())), preferred_element_type=F32)


def tn(a, b):
    return lax.dot_general(a, b, (((0,), (0,)), ((), ())), preferred_element_type=F32)


def split(v):
    high = v.astype(BF16)
    return high, (v - high.astype(F32)).astype(BF16)


def step_kernel(
    tok_ref, gain_ref, wq_ref, wk_ref, wv_ref, wg_ref, gin_ref, gf_ref, bias_ref, wo_ref,
    mem_ref, norm_ref, stab_ref, pk_ref, pv_ref, pin_ref, pf_ref, acc_ref,
    terms_ref, mem_out, norm_out, stab_out, keys_ref, values_ref,
    wbuf, swap, wob, tok_own, tok_mid, tokbuf, tg, pbuf, rbuf, sbuf, srecv, memv, gin_v, gf_v, gbuf, ebuf,
    gain_v, norm_v, stab_v, pk_v, pv_v, pin_v, pf_v, acc_v, bias_v, coef, norm8,
    loc_sem, xs_sem, xr_sem, ws_sem, wr_sem, fs_sem, fr_sem, ys_sem, yr_sem, ts_sem, tr_sem, rs_sem, rr_sem, ss_sem, sr_sem,
    gs_sem, gr_sem, es_sem, er_sem,
):
    z, x = lax.axis_index("z"), lax.axis_index("x")
    y, c = lax.axis_index("y"), lax.axis_index("c")
    j = y * NC + c
    right, left = lax.rem(x + 1, NX), lax.rem(x + NX - 1, NX)
    opposite = lax.rem(x + 2, NX)
    zs = [lax.rem(z + d, NZ) for d in range(NZ)]
    js = [lax.rem(j + d, NJ) for d in range(NJ)]
    ys = [lax.rem(y + d, NY) for d in range(NY)]
    self_tok = j == z
    even = lax.rem(z, 2)
    odd = 1 - even
    partner = z + 1 - 2 * even
    base = z - even

    def at_x(other):
        return (z, other, y, c)

    def at_z(other):
        return (other, x, y, c)

    def at_y(other):
        return (z, x, other, c)

    def at_zj(other, tp):
        return (other, x, lax.div(tp, NC), lax.rem(tp, NC))

    def rdma(src, dst, ssem, rsem, dev):
        return pltpu.make_async_remote_copy(
            src_ref=src, dst_ref=dst, send_sem=ssem, recv_sem=rsem,
            device_id=dev, device_id_type=MESH,
        )

    own_cols = pl.ds(pl.multiple_of(even * DK, DK), DK)
    other_cols = pl.ds(pl.multiple_of(odd * DK, DK), DK)

    def wblock(piece, owner, start, size):
        if piece < 8:
            proj, own = PIECES[piece]
            first = pl.multiple_of(owner * 128 + start * 32, 32)
            return wbuf.at[proj, even if own else odd, pl.ds(first, size * 32), :]
        cols = pl.ds(pl.multiple_of(owner * 128, 128), 128)
        return wob.at[pl.ds(start * 128, size * 128), cols]

    feats = pl.ds(pl.multiple_of(z * 512, 512), 512)
    moves = (
        (wq_ref.at[:, own_cols], wblock(0, x, 0, 4)), (wk_ref.at[:, own_cols], wblock(1, x, 0, 4)),
        (wv_ref.at[:, own_cols], wblock(2, x, 0, 4)), (wg_ref.at[:, own_cols], wblock(6, x, 0, 4)),
        (wq_ref.at[:, other_cols], swap.at[0]), (wk_ref.at[:, other_cols], swap.at[1]),
        (wv_ref.at[:, other_cols], swap.at[2]), (wg_ref.at[:, other_cols], swap.at[3]),
        (wo_ref, wblock(8, x, 0, 4)), (tok_ref, tok_own), (gin_ref.at[:, feats], gin_v), (gf_ref.at[:, feats], gf_v), (mem_ref, mem_out),
        (gain_ref, gain_v), (norm_ref, norm_v), (stab_ref, stab_v), (pk_ref, pk_v), (pv_ref, pv_v),
        (pin_ref, pin_v), (pf_ref, pf_v), (acc_ref, acc_v), (bias_ref, bias_v),
    )
    local = [pltpu.make_async_copy(src, dst, loc_sem.at[i]) for i, (src, dst) in enumerate(moves)]
    for i in (0, 9, 4, 1, 2, 5, 6, 7, 3, 15, 18, 19, 20, 13, 14, 16, 17, 10, 11, 21, 8, 12):
        local[i].start()

    barrier = pltpu.get_barrier_semaphore()

    def greet(dev):
        pl.semaphore_signal(barrier, inc=1, device_id=dev, device_id_type=MESH)

    greet(at_x(right))
    greet(at_x(left))
    for d in range(1, NZ):
        greet(at_z(zs[d]))
        greet((zs[d], x, y, 1 - c))
    for d in range(1, NJ):
        greet(at_zj(z, js[d]))
    pl.semaphore_wait(barrier, 23)

    def direct(p):
        return [
            rdma(wblock(p, x, 0, 4), wblock(p, x, 0, 4), xs_sem.at[p, 0], xr_sem.at[p, 0], at_x(right)),
            rdma(wblock(p, x, 0, 4), wblock(p, x, 0, 4), xs_sem.at[p, 1], xr_sem.at[p, 1], at_x(left)),
        ]

    def onward(p):
        return [
            rdma(wblock(p, left, 0, 2), wblock(p, left, 0, 2), xs_sem.at[p, 2], xr_sem.at[p, 2], at_x(right)),
            rdma(wblock(p, right, 2, 2), wblock(p, right, 2, 2), xs_sem.at[p, 3], xr_sem.at[p, 3], at_x(left)),
        ]

    def arrive(p, which):
        owner, start, size = ((left, 0, 4), (right, 0, 4), (opposite, 0, 2), (opposite, 2, 2))[which]
        block = wblock(p, owner, start, size)
        rdma(block, block, xs_sem.at[p, which], xr_sem.at[p, which], at_x(left)).wait_recv()

    sent = []

    def go(copies):
        for copy in copies:
            copy.start()
            sent.append(copy)

    def give(proj):
        mine = wbuf.at[proj, even, pl.ds(pl.multiple_of(x * 128, 128), 128), :]
        return rdma(swap.at[proj], mine, ws_sem.at[proj], wr_sem.at[proj], at_z(partner))

    def send(piece):
        if piece < 8:
            proj, own = PIECES[piece]
            if own:
                local[proj].wait()
            else:
                block = wblock(piece, x, 0, 4)
                rdma(swap.at[proj], block, ws_sem.at[proj], wr_sem.at[proj], at_z(partner)).wait_recv()
        else:
            local[8].wait()
        go(direct(piece))

    def forward(p):
        arrive(p, 0)
        arrive(p, 1)
        go(onward(p))
        if p < 5:
            send(p + 3)

    send(0)
    local[9].wait()
    go([rdma(tok_own, tok_mid.at[y], ys_sem.at[d], yr_sem.at[y], at_y(ys[d])) for d in (2, 1, 3)])
    relay_tok = []

    def spread(d):
        block = tok_own if d == 0 else tok_mid.at[ys[d]]
        if d:
            rdma(tok_own, block, ys_sem.at[d], yr_sem.at[ys[d]], at_y(ys[d])).wait_recv()
        same, cross = 2 * ys[d] + even, 2 * ys[d] + odd
        first = rdma(block, tokbuf.at[c, z], ts_sem.at[2 * d], tr_sem.at[z], at_z(same))
        go([rdma(block, tokbuf.at[c, z], ts_sem.at[2 * d + 1], tr_sem.at[z], at_z(cross))])
        relay_tok.append((first, same))

        @pl.when(same != z)
        def _():
            first.start()

        @pl.when(same == z)
        def _():
            tokbuf[c, z] = block[...]

    spread(0)
    for proj in range(4):
        local[4 + proj].wait()
        go([give(proj)])
        if proj < 2:
            send(proj + 1)

    for i in (15, 18, 19, 20):
        local[i].wait()
    taken = acc_v[...]
    stab = stab_v[...]
    logs, run = [], None
    for i in range(4):
        f = jnp.where(i < taken, log_sigmoid(pf_v[i]), 0.0)
        run = f if run is None else run + f
        logs.append(run)
    ends = [run - logs[i] + pin_v[i] for i in range(4)]
    stab_new = run + stab
    for i in range(4):
        stab_new = jnp.where(i < taken, jnp.maximum(stab_new, ends[i]), stab_new)
    stab_out[...] = stab_new
    for i in range(4):
        w = jnp.where(i < taken, jnp.exp(ends[i] - stab_new), 0.0) * (DK**-0.5)
        for h in range(2):
            coef[4 * h + i : 4 * h + i + 1, :] = w[h : h + 1]
    coef[8:10, :] = jnp.exp(run + stab - stab_new)
    coef[10:16, :] = jnp.zeros((6, 8), F32)
    coef_lane = lax.broadcasted_iota(jnp.int32, (16, 8), 1)
    for i in (12, 14, 16, 17):
        local[i].wait()

    def update(s, carry_in):
        col = jnp.sum(jnp.where(coef_lane == s, coef[...], 0.0), axis=1, keepdims=True)
        for h in range(2):
            cols = slice(h * DK, (h + 1) * DK)
            weighted = pk_v[s, :, cols].astype(F32) * col[4 * h : 4 * h + 4]
            carry = col[8 + h : 9 + h]
            high, low = split(weighted)
            vals = pv_v[s, :, cols]
            new = carry * mem_out[s, h] + (tn(high, vals) + tn(low, vals))
            mem_out[s, h] = new
            memv[s, h] = new.astype(BF16)
            row = carry * norm_v[s, h : h + 1] + jnp.sum(weighted, axis=0, keepdims=True)
            norm_out[s, h : h + 1] = row
            norm8[h, pl.ds(s, 1), :] = row
        return carry_in

    forward(0)

    for d in (1, 3, 2):
        spread(d)

    forward(1)
    lax.fori_loop(0, 2, update, 0)
    forward(2)
    lax.fori_loop(2, 4, update, 0)
    forward(3)
    lax.fori_loop(4, 6, update, 0)
    forward(4)
    lax.fori_loop(6, 8, update, 0)
    local[13].wait()

    def gains_of(plane):
        rows = [gain_v[pl.ds(4 * (base + plane) + r, 1), :] for r in range(4)]
        return jnp.concatenate(rows, axis=1)

    def crossing(core, slot):
        block = tokbuf.at[core, slot]
        return rdma(block, block, fs_sem.at[slot], fr_sem.at[slot], (z, x, y, 1 - c))

    def scale_block(core, slot, gains):
        scaled = (tokbuf[core, slot].astype(F32) * gains).astype(BF16)
        tg[core, pl.ds(pl.multiple_of(slot * ROWS, ROWS), ROWS), :] = scaled

    near_first = (0, 1, 7, 2, 6, 3, 5, 4)
    own_gains = gains_of(c)
    for d in near_first:
        slot = zs[d]
        if d:
            rdma(tok_own, tokbuf.at[c, slot], ts_sem.at[0], tr_sem.at[slot], at_z(slot)).wait_recv()
        go([crossing(c, slot)])
        scale_block(c, slot, own_gains)
    forward(5)
    other_gains = gains_of(1 - c)
    for d in near_first:
        slot = zs[d]
        crossing(1 - c, slot).wait_recv()
        scale_block(1 - c, slot, other_gains)
    far_first = (4, 3, 5, 2, 6, 1, 7)
    def hop(p, block, slot, to):
        return rdma(block, rbuf.at[p, slot], rs_sem.at[p, slot], rr_sem.at[p, slot], at_z(zs[to]))

    def landed(p, slot):
        hop(p, pbuf.at[p, z], slot, 1).wait_recv()
        return rbuf[p, slot].astype(F32)

    def project(p):
        for piece in range(8):
            if PIECES[piece][0] == p:
                arrive(piece, 2)
                arrive(piece, 3)
        part = jnp.dot(tg[0], wbuf[p, 0], preferred_element_type=F32)
        part = part + jnp.dot(tg[1], wbuf[p, 1], preferred_element_type=F32)
        pbuf[p] = part.astype(BF16).reshape(NZ, ROWS, DK)
        if p >= RELAYED:
            go([hop(p, pbuf.at[p, zs[d]], d, d) for d in far_first])
            return
        ahead, back = (2, 6) if p % 2 == 0 else (6, 2)
        go([
            hop(p, pbuf.at[p, zs[4]], 4, ahead),
            hop(p, pbuf.at[p, zs[3]], 3, 2),
            hop(p, pbuf.at[p, zs[5]], 5, 6),
            hop(p, pbuf.at[p, zs[back]], back, back),
        ])

    def pass_on(p, target, slot):
        total = pbuf[p, zs[target]].astype(F32) + landed(p, slot)
        pbuf[p, zs[target]] = total.astype(BF16)
        go([hop(p, pbuf.at[p, zs[target]], target, target)])

    def relay(p):
        pass_on(p, 1, 3)
        pass_on(p, 7, 5)
        pass_on(p, 2 if p % 2 == 0 else 6, 4)

    def collect(p):
        mine = pbuf[p, z].astype(F32)
        for slot in (2, 6) if p < RELAYED else (2, 6, 4):
            mine = mine + landed(p, slot)
        other = landed(p, 1)
        for slot in (7,) if p < RELAYED else (7, 3, 5):
            other = other + landed(p, slot)
        mine = (mine * scale_col).astype(BF16)
        other = (other * scale_col).astype(BF16)
        return jnp.where(even == 0, mine, other), jnp.where(even == 0, other, mine)

    small = []

    def send_small():
        row8 = lax.broadcasted_iota(jnp.int32, (8, 16), 0)
        lane16 = lax.broadcasted_iota(jnp.int32, (8, 16), 1)
        pick_in = jnp.where((row8 < 2) & (lane16 == 2 * j + row8), 1.0, 0.0).astype(BF16)
        pick_f = jnp.where((row8 >= 2) & (row8 < 4) & (lane16 == 2 * j + row8 - 2), 1.0, 0.0).astype(BF16)
        local[10].wait()
        local[11].wait()
        gates8 = (
            jnp.dot(pick_in, gin_v[...], preferred_element_type=F32)
            + jnp.dot(pick_f, gf_v[...], preferred_element_type=F32)
        ).astype(BF16)
        ones8 = jnp.full((8, 512), 1.0, BF16)
        row_all = lax.broadcasted_iota(jnp.int32, (8, NZ * ROWS), 0)
        sbuf[...] = jnp.zeros_like(sbuf)
        raw = tokbuf[even].astype(F32).reshape(NZ * ROWS, 512)
        high, low = split(raw * raw)
        squares = nt(ones8, high) + nt(ones8, low)
        rows = jnp.where(row_all == 4, squares, nt(gates8, tg[even]))
        for i in range(NZ):
            sbuf[i, :, 0:ROWS] = rows[:, i * ROWS : (i + 1) * ROWS]
        small.extend(
            rdma(sbuf.at[zs[d]], srecv.at[d], ss_sem.at[d], sr_sem.at[d], at_z(zs[d])) for d in far_first
        )
        go(small)

    project(0)
    forward(6)
    project(1)
    forward(7)
    send(8)
    project(2)
    relay(0)
    send_small()
    relay(1)
    project(3)

    for copy in small:
        copy.wait_recv()
    sums = sbuf[z]
    for d in range(1, NZ):
        sums = sums + srecv[d]
    scale_row = lax.rsqrt(sums[4:5, 0:ROWS] / D + EPS)
    ri = lax.broadcasted_iota(jnp.int32, (ROWS, ROWS), 0)
    ci = lax.broadcasted_iota(jnp.int32, (ROWS, ROWS), 1)
    eye = ri == ci
    same = lax.div(ri, 4) == lax.div(ci, 4)
    causal = same & (ci <= ri)
    anti = same & (ri <= ci)

    def to_col(row):
        return jnp.sum(jnp.where(eye, row, 0.0), axis=1, keepdims=True)

    scale_col = to_col(scale_row)
    seq_of_row = lax.div(lax.broadcasted_iota(jnp.int32, (ROWS, 8), 0), 4)
    seq_lane = lax.broadcasted_iota(jnp.int32, (ROWS, 8), 1)
    own_seq = seq_of_row == seq_lane
    row_seq = lax.div(lax.broadcasted_iota(jnp.int32, (ROWS, DK), 0), 4)

    queries = collect(0)
    carried_rows = []
    for h in range(2):
        read = jnp.zeros((ROWS, DK), F32)
        for s in range(8):
            part = jnp.dot(queries[h], memv[s, h], preferred_element_type=F32)
            read = jnp.where(row_seq == s, part, read)
        carried_rows.append(read)
    keys = collect(1)
    values = collect(2)
    for h in range(2):
        keys_ref[:, h * DK : (h + 1) * DK] = keys[h]
        values_ref[:, h * DK : (h + 1) * DK] = values[h]

    local[21].wait()
    bias_lane = lax.broadcasted_iota(jnp.int32, (1, 16), 1)
    hidden = []
    for h in range(2):
        q, k, v = queries[h], keys[h], values[h]
        bias = jnp.sum(jnp.where(bias_lane == 2 * j + h, bias_v[...], 0.0), axis=1, keepdims=True)
        in_row = sums[h : h + 1, 0:ROWS] * scale_row
        f_row = log_sigmoid(sums[2 + h : 3 + h, 0:ROWS] * scale_row + bias)
        f_col = to_col(f_row)
        b_col = jnp.sum(jnp.where(causal, f_row, 0.0), axis=1, keepdims=True)
        b_row = jnp.sum(jnp.where(anti, f_col, 0.0), axis=0, keepdims=True)
        within = jnp.where(causal, b_col - b_row + in_row, -jnp.inf)
        stab_col = jnp.sum(jnp.where(own_seq, stab_out[h : h + 1, :], 0.0), axis=1, keepdims=True)
        g_col = b_col + stab_col
        level = jnp.maximum(g_col, jnp.max(within, axis=1, keepdims=True))
        u = jnp.exp(g_col - level)
        w = nt(q, k) * (DK**-0.5) * jnp.where(causal, jnp.exp(within - level), 0.0)
        w_high, w_low = split(w)
        n_high, n_low = split(norm8[h])
        q_norm = jnp.sum(jnp.where(own_seq, nt(q, n_high) + nt(q, n_low), 0.0), axis=1, keepdims=True)
        num = u * carried_rows[h] + (
            jnp.dot(w_high, v, preferred_element_type=F32) + jnp.dot(w_low, v, preferred_element_type=F32)
        )
        den = u * q_norm + jnp.sum(w, axis=1, keepdims=True)
        hidden.append(num / jnp.maximum(jnp.abs(den), 1.0))

    arrive(8, 0)
    arrive(8, 1)
    go(onward(8))
    pre = collect(3)
    for h in range(2):
        gbuf[h, z] = (jax.nn.sigmoid(pre[h].astype(F32)) * hidden[h]).astype(BF16)
    go([
        rdma(gbuf.at[h, z], gbuf.at[h, z], gs_sem.at[h, d], gr_sem.at[h, d], at_z(zs[d]))
        for d in far_first
        for h in range(2)
    ])
    arrive(8, 2)
    arrive(8, 3)

    for d in (3, 5, 1, 7, 2, 6, 4, 0):
        slot = zs[d]
        out = jnp.zeros((ROWS, 512), F32)
        for h in range(2):
            if d:
                came = NZ - d
                rdma(
                    gbuf.at[h, slot], gbuf.at[h, slot], gs_sem.at[h, came], gr_sem.at[h, came], at_z(slot)
                ).wait_recv()
            out = out + jnp.dot(gbuf[h, slot], wob[h * DK : (h + 1) * DK, :], preferred_element_type=F32)
        ebuf[slot] = out.astype(BF16)
        out = rdma(ebuf.at[slot], terms_ref.at[j], es_sem.at[d], er_sem.at[j], at_zj(slot, z))
        if d:
            go([out])
        else:
            own_out = out

            @pl.when(jnp.logical_not(self_tok))
            def _():
                own_out.start()

            @pl.when(self_tok)
            def _():
                terms_ref[j] = ebuf[slot]

    for d in range(NJ):
        slot = js[d]
        came = rdma(ebuf.at[0], terms_ref.at[slot], es_sem.at[d], er_sem.at[slot], at_zj(z, slot))
        if d:
            came.wait_recv()
        else:
            @pl.when(jnp.logical_not(self_tok))
            def _(came=came):
                came.wait_recv()

    for copy in sent:
        copy.wait_send()
    for copy, same in relay_tok:
        @pl.when(same != z)
        def _(copy=copy):
            copy.wait_send()

    @pl.when(jnp.logical_not(self_tok))
    def _():
        own_out.wait_send()


def finish_kernel(terms, mem, norm, stab, keys, values, mixed, mem_o, norm_o, stab_o, keys_o, values_o, total_v, sem):
    pairs = ((mem, mem_o), (norm, norm_o), (stab, stab_o), (keys, keys_o), (values, values_o), (total_v, mixed))
    copies = [pltpu.make_async_copy(src, dst, sem.at[i]) for i, (src, dst) in enumerate(pairs)]
    for copy in copies[1:5]:
        copy.start()
    total = terms[0].astype(F32)
    for i in range(1, NJ):
        total = total + terms[i].astype(F32)
    total_v[...] = total.astype(BF16)
    copies[0].start()
    copies[5].start()
    for copy in copies:
        copy.wait()


def step(*args):
    args = [pltpu.with_memory_space_constraint(a, pltpu.HBM) for a in args]
    hbm = pl.BlockSpec(memory_space=pltpu.HBM)
    vmem = pl.BlockSpec(memory_space=pltpu.VMEM)
    dma = pltpu.SemaphoreType.DMA
    block = lambda *lead: pltpu.VMEM((*lead, ROWS, 512), BF16)
    shape = jax.ShapeDtypeStruct
    outs = [
        shape((NJ, ROWS, 512), BF16), shape((8, 2, DK, DK), F32), shape((8, 2, DK), F32),
        shape((2, 8), F32), shape((ROWS, 512), BF16), shape((ROWS, 512), BF16),
    ]
    parts = pl.pallas_call(
        step_kernel,
        in_specs=[hbm] * 18,
        out_specs=[vmem] * 6,
        out_shape=outs,
        scratch_shapes=[
            pltpu.VMEM((4, 2, 512, DK), BF16),
            pltpu.VMEM((4, 128, DK), BF16),
            pltpu.VMEM((512, 512), BF16),
            block(),
            block(NY),
            block(2, NZ),
            pltpu.VMEM((2, 256, 512), BF16),
            pltpu.VMEM((4, NZ, ROWS, DK), BF16),
            pltpu.VMEM((4, NZ, ROWS, DK), BF16),
            pltpu.VMEM((NZ, 8, 128), F32),
            pltpu.VMEM((NZ, 8, 128), F32),
            pltpu.VMEM((8, 2, DK, DK), BF16),
            pltpu.VMEM((16, 512), BF16),
            pltpu.VMEM((16, 512), BF16),
            pltpu.VMEM((2, NZ, ROWS, DK), BF16),
            block(NZ),
            pltpu.VMEM((32, 128), F32),
            pltpu.VMEM((8, 2, DK), F32),
            pltpu.VMEM((2, 8), F32),
            pltpu.VMEM((8, 4, 512), BF16),
            pltpu.VMEM((8, 4, 512), BF16),
            pltpu.VMEM((4, 2, 8), F32),
            pltpu.VMEM((4, 2, 8), F32),
            pltpu.VMEM((1, 8), jnp.int32),
            pltpu.VMEM((1, 16), F32),
            pltpu.VMEM((16, 8), F32),
            pltpu.VMEM((2, 8, DK), F32),
            dma((22,)), dma((9, 4)), dma((9, 4)), dma((4,)), dma((4,)), dma((8,)), dma((8,)),
            dma((4,)), dma((4,)), dma((8,)), dma((8,)),
            dma((4, 8)), dma((4, 8)), dma((8,)), dma((8,)), dma((2, 8)), dma((2, 8)), dma((8,)), dma((8,)),
        ],
        compiler_params=pltpu.CompilerParams(
            collective_id=0, has_side_effects=True, vmem_limit_bytes=24 * 1024 * 1024
        ),
        name="step",
    )(*args)
    return pl.pallas_call(
        finish_kernel,
        in_specs=[vmem] + [pl.BlockSpec(memory_space=pl.ANY)] * 5,
        out_specs=[hbm] * 6,
        out_shape=[shape((ROWS, 512), BF16)] + outs[1:],
        scratch_shapes=[pltpu.VMEM((ROWS, 512), BF16), dma((6,))],
        name="finish",
        compiler_params=pltpu.CompilerParams(vmem_limit_bytes=4 * 1024 * 1024),
    )(*[pltpu.with_memory_space_constraint(part, pltpu.VMEM) for part in parts])


def body(
    tokens, norm_gain, query_weight, key_weight, value_weight, outgate_weight, ingate_weight,
    forget_weight, forget_bias, output_weight, state_memory, state_normaliser, state_stabiliser,
    past_keys, past_values, past_ingate, past_forget, accepted,
):
    mixed, memory, normaliser, stab_t, keys, values = step(
        tokens, norm_gain.reshape(32, 128), query_weight, key_weight, value_weight, outgate_weight,
        ingate_weight.T, forget_weight.T, forget_bias.reshape(1, 16), output_weight,
        state_memory, state_normaliser, state_stabiliser.T, past_keys, past_values,
        past_ingate.transpose(1, 2, 0), past_forget.transpose(1, 2, 0), accepted.reshape(1, 8),
    )
    return (mixed, memory, normaliser, stab_t.T, keys, values)


def solution(mesh):
    torus = Mesh(mesh.devices.reshape(NZ, NX, NY, NC), ("z", "x", "y", "c"))
    kv, tp = ("z", "x"), ("y", "c")
    in_specs = (
        P(kv, tp), P(), P(kv, tp), P(kv, tp), P(kv, tp), P(kv, tp), P(), P(), P(), P(tp, kv),
        P(kv, tp, None, None), P(kv, tp, None), P(kv, tp), P(kv, None, tp), P(kv, None, tp),
        P(kv, None, tp), P(kv, None, tp), P(kv),
    )
    out_specs = (
        P(kv, tp), P(kv, tp, None, None), P(kv, tp, None), P(kv, tp), P(kv, tp), P(kv, tp),
    )
    return jax.shard_map(body, mesh=torus, in_specs=in_specs, out_specs=out_specs, check_vma=False)
```
